128 devices in a mesh: sp: 64 (over z, y, x), tp: 2 (over core).
Axes of the slice: x: 4, y: 4, z: 4, core: 2. Of those that a mesh axis runs over, the one named last changes fastest.
Arguments:
- queries: bfloat16 [16384, 1024], P('sp', 'tp'), may hold values from -7 to 7
- keys: bfloat16 [16384, 256], P('sp', 'tp'), may hold values from -6 to 6
- values: bfloat16 [16384, 256], P('sp', 'tp'), may hold values from -6 to 6
- q_gain: float32 [64], replicated, may hold values from 0.5 to 5
- k_gain: float32 [64], replicated, may hold values from 0.5 to 5
- resid: bfloat16 [16384, 2048], P(('sp', 'tp')), may hold values from -6 to 6
- out_weight: bfloat16 [1024, 2048], P('tp'), may hold values from -0.1875 to 0.1875
- post_gain: float32 [2048], replicated, may hold values from 0.1 to 1.9
- ffn_gain: float32 [2048], replicated, may hold values from 0.1 to 1.9
- post_ffn_gain: float32 [2048], replicated, may hold values from 0.1 to 1.9
- gate_w: bfloat16 [64, 2048, 3584], P('sp', None, 'tp'), may hold values from -0.125 to 0.125
- up_w: bfloat16 [64, 2048, 3584], P('sp', None, 'tp'), may hold values from -0.125 to 0.125
- down_w: bfloat16 [64, 3584, 2048], P('sp', 'tp'), may hold values from -0.09375 to 0.09375
- route_ids: int32 [16384, 2], P(('sp', 'tp')), may hold values from 0 to 63, all different within a row; in each aligned block of 128 rows (0 to 127, 128 to 255, ...) at most 6 rows name the same one
- route_w: float32 [16384, 2], P(('sp', 'tp')), may hold values from 0.2 to 1
Outputs:
- layer_out: bfloat16 [16384, 2048], P(('sp', 'tp'))
The draws below stay inside these ranges and needn't reach their ends.
Inputs may be any that keep to these rules, and one draw needn't show every extreme that they name: `route_ids`: each row names 2 different experts. In each aligned block of 128 rows (the rows of one device) no expert is named more than 6 times, a bound that some blocks reach.
All inputs are finite; a program needn't handle non-finite values.
Results may differ from the reference program's by a relative error of at most 0.017.
The reference program's roundings to bfloat16 on the way count: a program that leaves them out, or rounds other values in their place, can miss the bound.
Values may be sent and summed in bfloat16 or wider, within the bound.
A program may use at most 128 MiB of HBM per device.

```python
import math
import jax
import jax.numpy as jnp
import numpy as np
from jax import lax

D = 2048
HEADS = 16
KV_HEADS = 4
HEAD_DIM = 64
FF_E = 3584
GRID_W = 64
TOP = 2
TOKENS = 16384
EXPERTS = 64
ROWS_DEV = 128
CAP = 6
N_SP = 64
N_TP = 2


def base_keys(key):
    fresh = jax.random.normal(jax.random.fold_in(key, 11), (TOKENS, KV_HEADS * HEAD_DIM), jnp.float32)
    return jnp.clip(fresh, -6.0, 6.0)


def draw_keys(key, part):
    return base_keys(key).astype(jnp.bfloat16)


def draw_queries(key, part):
    fresh = jax.random.normal(jax.random.fold_in(key, 12), (TOKENS, HEADS, HEAD_DIM), jnp.float32)
    fresh = jnp.clip(fresh, -6.0, 6.0)
    return fresh.reshape(TOKENS, HEADS * HEAD_DIM).astype(jnp.bfloat16)


def gain_draw(key, salt):
    spread = jax.random.uniform(jax.random.fold_in(key, salt), (HEAD_DIM,), jnp.float32, math.log(0.5), math.log(2.0))
    return jnp.exp(spread)


def draw_q_gain(key, part):
    return gain_draw(key, 13)


def draw_k_gain(key, part):
    return gain_draw(key, 14)


def levels(stream_key, extent, shards, smallest, largest):
    factor_of, own = 1.0, jax.random.fold_in(stream_key, 6)
    for position, blocks in shards:
        heights = jnp.exp(jax.random.uniform(jax.random.fold_in(own, position), (blocks,), jnp.float32, smallest / len(shards), largest / len(shards)))
        factor_of = factor_of * jnp.repeat(heights, extent[position] // blocks).reshape([-1 if axis == position else 1 for axis in range(len(extent))])
    return factor_of


def routed_block(rng, own, number, rows, count, top, reach, skew):
    ranking = jax.random.permutation(rng, count)
    heavy_load, common = portions_of(count, rows * top, reach, skew, True), portions_of(count, rows * top, reach, skew, False)
    places = jnp.arange(count)

    def named(lengths, turn):
        used = int((lengths > 0).sum())
        fixed = max(1, used // 4)
        shifted = fixed + (places - fixed + turn * (used - fixed)) % max(1, count - fixed)
        return jnp.zeros((count,), jnp.int32).at[ranking[jnp.where(places < fixed, places, shifted)]].set(jnp.asarray(lengths, jnp.int32))

    lengths = jnp.where(number % 4 == 0, named(heavy_load, number // 4), named(common, number - number // 4 - 1))
    mixed = jax.random.permutation(jax.random.fold_in(own, 3), count)
    source_of, receiver = mixed[0:count // 2 * 2:2], mixed[1:count // 2 * 2:2]
    slack = jnp.minimum(lengths[source_of] - 1, reach - lengths[receiver]) // 2
    slack = jnp.where((source_of == ranking[0]) | (receiver == ranking[0]) | (lengths[receiver] == 0), 0, jnp.maximum(slack, 0))
    shifted = jax.random.randint(jax.random.fold_in(own, 4), (count // 2,), 0, 1 << 20) % (slack + 1)
    lengths = lengths.at[source_of].add(-shifted).at[receiver].add(shifted)
    labels = jnp.searchsorted(jnp.cumsum(lengths), jnp.arange(rows * top), side="right").astype(jnp.int32)
    listing = labels.reshape(top, rows).T
    listing = listing[jax.random.permutation(jax.random.fold_in(own, 1), rows)]
    turn = jax.random.randint(jax.random.fold_in(own, 2), (rows, 1), 0, top)
    return jnp.take_along_axis(listing, (jnp.arange(top)[None, :] + turn) % top, axis=1)


def portions_of(amount, total, limit, slope, full):
    loads = [(1 << 20) // math.isqrt(standing ** slope) + 1 for standing in range(1, amount + 1)]
    largest = limit if full else min(limit, max(-(-total // amount), total * loads[0] // sum(loads)))
    least = 1 if total - largest >= amount - 1 else 0
    holding, rest = [largest] + [least] * (amount - 1), total - largest - least * (amount - 1)
    while rest > 0:
        candidates = [i for i in range(1, amount) if holding[i] < largest] or [i for i in range(1, amount) if holding[i] < limit]
        mass, remaining = sum([loads[i] for i in candidates]), rest
        for i in candidates:
            addition = min(limit - holding[i], max(1, remaining * loads[i] // mass), rest)
            holding[i] = holding[i] + addition
            rest = rest - addition
    return np.array(holding)


def noise(key, shape, deviation, most, cuts=(), held_as=jnp.bfloat16):
    array = jax.random.normal(key, shape, jnp.float32) * deviation
    if len(cuts) > 0:
        array = levels(key, shape, cuts, -0.22, 0.18) * array
    return jnp.clip(array, min=-most, max=most).astype(held_as)


def setup_inputs(seed: int = 0) -> dict:
    streams_of = jax.random.split(jax.random.key(seed), 16)
    queries = draw_queries(jax.random.fold_in(streams_of[15], 71), 0)
    keys = draw_keys(jax.random.fold_in(streams_of[15], 71), 0)
    values = noise(streams_of[2], (TOKENS, KV_HEADS * HEAD_DIM), 1.0, 6.0, ((0, 64), (1, 2)))
    q_gain = draw_q_gain(jax.random.fold_in(streams_of[15], 71), 0)
    k_gain = draw_k_gain(jax.random.fold_in(streams_of[15], 71), 0)
    resid = noise(streams_of[5], (TOKENS, D), 1.0, 6.0, ((0, 128),))
    out_weight = noise(streams_of[6], (HEADS * HEAD_DIM, D), (HEADS * HEAD_DIM) ** -0.5, 0.1875, ((0, 2),))
    post_gain = jnp.clip(1.0 + 0.18 * jax.random.normal(streams_of[7], (D,), jnp.float32), 0.1, 1.9)
    ffn_gain = jnp.clip(1.0 + 0.18 * jax.random.normal(streams_of[8], (D,), jnp.float32), 0.1, 1.9)
    post_ffn_gain = jnp.clip(1.0 + 0.18 * jax.random.normal(streams_of[9], (D,), jnp.float32), 0.1, 1.9)
    gate_w = noise(streams_of[10], (EXPERTS, D, FF_E), D ** -0.5, 0.125, ((0, 64), (2, 2)))
    up_w = noise(streams_of[11], (EXPERTS, D, FF_E), D ** -0.5, 0.125, ((0, 64), (2, 2)))
    down_w = noise(streams_of[12], (EXPERTS, FF_E, D), FF_E ** -0.5, 0.09375, ((0, 64), (1, 2)))
    route_ids_keys = jax.random.split(jax.random.fold_in(streams_of[13], 1), TOKENS // ROWS_DEV)
    route_ids_turns = jax.random.permutation(jax.random.fold_in(streams_of[13], 3), TOKENS // ROWS_DEV)
    route_ids = jax.vmap(lambda own, number: routed_block(jax.random.fold_in(streams_of[13], 2), own, number, ROWS_DEV, EXPERTS, TOP, CAP, 1))(route_ids_keys, route_ids_turns).reshape((TOKENS, TOP))
    route_w = jnp.clip(0.2 + 0.8 * jax.random.uniform(streams_of[14], (TOKENS, TOP), jnp.float32) ** levels(streams_of[14], (TOKENS, TOP), ((0, 128),), -0.2, 0.2), 0.2, 1.0)
    return dict(queries=queries, keys=keys, values=values, q_gain=q_gain, k_gain=k_gain, resid=resid, out_weight=out_weight, post_gain=post_gain, ffn_gain=ffn_gain, post_ffn_gain=post_ffn_gain, gate_w=gate_w, up_w=up_w, down_w=down_w, route_ids=route_ids, route_w=route_w)


EPS = 1e-06
THETA = 10000.0

def qk_prepare(raw, gain, positions, head_count):
    count_rows = raw.shape[0]
    values32 = raw.astype(jnp.float32).reshape(count_rows, head_count, HEAD_DIM)
    normed = values32 * lax.rsqrt(lax.optimization_barrier(jnp.mean(values32 * values32, axis=-1, keepdims=True)) + EPS) * gain
    half_dim = HEAD_DIM // 2
    freqs = THETA ** (-jnp.arange(0, half_dim, 2, dtype=jnp.float32) / half_dim)
    grid_row = (positions // GRID_W).astype(jnp.float32)
    grid_col = (positions % GRID_W).astype(jnp.float32)
    angles = jnp.concatenate([grid_row[:, None] * freqs, grid_col[:, None] * freqs], axis=-1)
    cosine = jnp.cos(angles)[:, None, :]
    sine = jnp.sin(angles)[:, None, :]
    paired = normed.reshape(count_rows, head_count, half_dim, 2)
    first = paired[..., 0]
    second = paired[..., 1]
    turned = jnp.stack([first * cosine - second * sine, first * sine + second * cosine], axis=-1)
    return turned.reshape(count_rows, head_count * HEAD_DIM).astype(jnp.bfloat16)

def rms_scale(values32, gain):
    return values32 * lax.rsqrt(lax.optimization_barrier(jnp.mean(values32 * values32, axis=-1, keepdims=True)) + EPS) * gain

def reference(queries, keys, values, q_gain, k_gain, resid, out_weight, post_gain, ffn_gain, post_ffn_gain, gate_w, up_w, down_w, route_ids, route_w):
    positions = jnp.arange(TOKENS, dtype=jnp.int32)
    group_size = HEADS // KV_HEADS
    scale_factor = HEAD_DIM ** (-0.5)
    query_n = qk_prepare(queries, q_gain, positions, HEADS).reshape(TOKENS // 128, 128, KV_HEADS, group_size, HEAD_DIM)
    key_n = qk_prepare(keys, k_gain, positions, KV_HEADS).reshape(TOKENS, KV_HEADS, HEAD_DIM).astype(jnp.float32)
    value_n = values.reshape(TOKENS, KV_HEADS, HEAD_DIM).astype(jnp.float32)

    def attend(block):
        scores = jnp.einsum('qhgd,khd->hgqk', block.astype(jnp.float32), key_n) * scale_factor
        top_score = lax.optimization_barrier(jnp.max(scores, axis=-1, keepdims=True))
        expo = jnp.exp(scores - top_score)
        total = lax.optimization_barrier(jnp.sum(expo, axis=-1))
        weights = lax.optimization_barrier(expo.astype(jnp.bfloat16)).astype(jnp.float32)
        summed = jnp.einsum('hgqk,khd->qhgd', weights, value_n)
        result = summed / jnp.transpose(total, (2, 0, 1))[..., None]
        return result.astype(jnp.bfloat16).reshape(128, HEADS * HEAD_DIM)
    attended = lax.map(attend, query_n).reshape(TOKENS, HEADS * HEAD_DIM)
    mixed = jnp.dot(attended, out_weight, preferred_element_type=jnp.float32)
    hidden_state = (resid.astype(jnp.float32) + rms_scale(mixed, post_gain)).astype(jnp.bfloat16)
    normed = rms_scale(hidden_state.astype(jnp.float32), ffn_gain).astype(jnp.bfloat16)
    bound = CAP * N_SP * N_TP
    pair_count = TOKENS * TOP
    pair_experts = route_ids.reshape(-1)
    padded_rows = jnp.concatenate([normed, jnp.zeros((1, D), jnp.bfloat16)], axis=0)
    part_width = FF_E // N_TP

    def expert_pass(expert):
        slots = jnp.nonzero(pair_experts == expert, size=bound, fill_value=pair_count)[0].astype(jnp.int32)
        token_ids = jnp.where(slots < pair_count, slots // TOP, TOKENS).astype(jnp.int32)
        rows_in = padded_rows[token_ids]
        gate = jnp.dot(rows_in, gate_w[expert], preferred_element_type=jnp.float32)
        upward = jnp.dot(rows_in, up_w[expert], preferred_element_type=jnp.float32)
        inner = (jax.nn.silu(gate) * upward).astype(jnp.bfloat16)
        down_here = down_w[expert]
        total = jnp.zeros((bound, D), jnp.float32)
        for part in range(N_TP):
            partial_sum = jnp.dot(inner[:, part * part_width:(part + 1) * part_width], down_here[part * part_width:(part + 1) * part_width], preferred_element_type=jnp.float32)
            total = total + lax.optimization_barrier(partial_sum.astype(jnp.bfloat16)).astype(jnp.float32)
        return (slots, total.astype(jnp.bfloat16))
    slot_table, results = lax.map(expert_pass, jnp.arange(EXPERTS, dtype=jnp.int32))
    placed = jnp.zeros((pair_count + 1, D), jnp.bfloat16).at[slot_table.reshape(-1)].set(results.reshape(-1, D))
    picked = placed[:pair_count].reshape(TOKENS, TOP, D).astype(jnp.float32)
    combined = lax.optimization_barrier(jnp.sum(route_w[:, :, None] * picked, axis=1))
    return (hidden_state.astype(jnp.float32) + rms_scale(combined, post_ffn_gain)).astype(jnp.bfloat16)
```

```python
import jax
import jax.numpy as jnp
from jax import lax
from jax.experimental import pallas as pl
from jax.experimental.pallas import tpu as pltpu
from jax.sharding import PartitionSpec as P

HEAD_DIM = 64
GRID_W = 64


EPS = 1e-06
THETA = 10000.0


def joined_along(pieces, dim):
    pieces = jnp.moveaxis(pieces, 0, dim)
    lengths = pieces.shape
    return pieces.reshape(*lengths[:dim], lengths[dim] * lengths[dim + 1], *lengths[dim + 2 :])


def work_in_pieces(value, axis, dim, work, out_dim):
    extent = value.shape[dim]
    pieces = jnp.split(value, 2, axis=dim) if extent % 2 == 0 else [value]
    initial = jnp.arange(lax.axis_size(axis)) * extent
    blocks = [lax.all_gather(piece, axis) for piece in pieces]
    made = [jax.vmap(work)(b, initial + k * (extent // len(pieces))) for k, b in enumerate(blocks)]
    return joined_along(jnp.concatenate(made, axis=out_dim + 1), out_dim)


def split_up(value, dim, devices):
    lengths = value.shape
    pieces = value.reshape(*lengths[:dim], devices, lengths[dim] // devices, *lengths[dim + 1 :])
    return jnp.moveaxis(pieces, dim, 0)


def summed_on_arrival(value, axis, dim):
    devices = lax.axis_size(axis)
    pieces = lax.all_to_all(split_up(value, dim, devices), axis, 0, 0, tiled=True)
    return jnp.sum(pieces.astype(jnp.float32), axis=0)


def qk_prepare(raw, gain, positions, head_count):
    count_rows = raw.shape[0]
    values32 = raw.astype(jnp.float32).reshape(count_rows, head_count, HEAD_DIM)
    normed = (
        values32 * lax.rsqrt(jnp.mean(values32 * values32, axis=-1, keepdims=True) + EPS) * gain
    )
    half_dim = HEAD_DIM // 2
    freqs = THETA ** (-jnp.arange(0, half_dim, 2, dtype=jnp.float32) / half_dim)
    grid_row = (positions // GRID_W).astype(jnp.float32)
    grid_col = (positions % GRID_W).astype(jnp.float32)
    angles = jnp.concatenate([grid_row[:, None] * freqs, grid_col[:, None] * freqs], axis=-1)
    cosine = jnp.cos(angles)[:, None, :]
    sine = jnp.sin(angles)[:, None, :]
    paired = normed.reshape(count_rows, head_count, half_dim, 2)
    first = paired[..., 0]
    second = paired[..., 1]
    turned = jnp.stack([first * cosine - second * sine, first * sine + second * cosine], axis=-1)
    return turned.reshape(count_rows, head_count * HEAD_DIM).astype(jnp.bfloat16)


def rms_scale(values32, gain):
    return values32 * lax.rsqrt(jnp.mean(values32 * values32, axis=-1, keepdims=True) + EPS) * gain


MESH_ID = pl.DeviceIdType.MESH
LIMIT = 2.0**100
QSCALE = 1.4426950408889634 / 8.0


def hops(d):
    return (0, 1, 2, 1)[d]


ORDER = sorted(range(64), key=lambda o: hops(o // 16) + hops(o // 4 % 4) + hops(o % 4))


def packed(start):
    words = []
    for g in range(16):
        w = 0
        for j in range(4):
            n = 4 * g + start + j
            w += (ORDER[n] if n < 64 else 0) * 64**j
        words.append(w)
    return words


def lookup(words, g):
    w = jnp.int32(words[0])
    for i in range(1, len(words)):
        w = jnp.where(g == i, jnp.int32(words[i]), w)
    return w


def pick(a, z, y, x):
    return jnp.where(a == 0, z, jnp.where(a == 1, y, x))


def source_of(offset, me):
    mz, my, mx = me // 16, (me // 4) % 4, me % 4
    cz = (mz + 4 - offset // 16) % 4
    cy = (my + 4 - (offset // 4) % 4) % 4
    cx = (mx + 4 - offset % 4) % 4
    return cz * 16 + cy * 4 + cx


def each_send(offset, me, act):
    mz, my, mx = me // 16, (me // 4) % 4, me % 4
    oz, oy, ox = offset // 16, (offset // 4) % 4, offset % 4
    src = source_of(offset, me)
    total = src // 16 + (src // 4) % 4 + src % 4
    kind, odd = total % 3, total % 2
    axes = [(kind + i) % 3 for i in range(3)]
    stride = [pick(a, 16, 4, 1) for a in axes]
    digit = [pick(a, oz, oy, ox) for a in axes]
    mine = [pick(a, mz, my, mx) for a in axes]

    def peer(i, step):
        return me + ((mine[i] + step) % 4 - mine[i]) * stride[i]

    none = offset == 0
    last = jnp.where(digit[2] > 0, 2, jnp.where(digit[1] > 0, 1, jnp.where(digit[0] > 0, 0, -1)))
    for i in range(3):

        @pl.when(i > last)
        def _():
            act(src, peer(i, 1), 2 * i)
            act(src, peer(i, 3), 2 * i + 1)

        @pl.when(jnp.logical_and(i == last, jnp.logical_and(digit[i] == 1, odd == 0)))
        def _():
            act(src, peer(i, 1), 2 * i)

        @pl.when(jnp.logical_and(i == last, jnp.logical_and(digit[i] == 3, odd == 1)))
        def _():
            act(src, peer(i, 3), 2 * i + 1)


def turned_heads(x, gain, cosine, sine):
    out = []
    for h in range(2):
        even, odd = x[64 * h : 64 * h + 32], x[64 * h + 32 : 64 * h + 64]
        squares = jnp.sum(even * even, axis=0, keepdims=True) + jnp.sum(odd * odd, axis=0, keepdims=True)
        scale = lax.rsqrt(squares * (1.0 / 64.0) + EPS)
        even, odd = even * scale * gain[0:32], odd * scale * gain[32:64]
        out.append(jnp.concatenate([even * cosine - odd * sine, even * sine + odd * cosine], axis=0))
    return out


def attention_kernel(
    q_ref, k_ref, v_ref, gains_ref, trig_ref, o_ref, den_ref, kv_out,
    qt, top, acc, kv, send_sem, recv_sem, out_sem,
):
    me, core = lax.axis_index("sp"), lax.axis_index("tp")
    mz, my, mx = me // 16, (me // 4) % 4, me % 4
    barrier = pltpu.get_barrier_semaphore()
    for stride, c in ((16, mz), (4, my), (1, mx)):
        for step in (1, 3):
            to = me + ((c + step) % 4 - c) * stride
            pl.semaphore_signal(barrier, inc=1, device_id=(to, core), device_id_type=MESH_ID)

    row = lax.broadcasted_iota(jnp.int32, (128, 128), 0)
    col = lax.broadcasted_iota(jnp.int32, (128, 128), 1)
    within = row % 64
    wanted = (row // 64) * 64 + 2 * (within % 32) + within // 32
    order = (col == wanted).astype(jnp.float32).astype(jnp.bfloat16)
    same = (col == row).astype(jnp.float32).astype(jnp.bfloat16)
    nt = (((1,), (1,)), ((), ()))
    cosine, sine = trig_ref[0:32, :], trig_ref[32:64, :]
    kt = turned_heads(
        lax.dot_general(order, k_ref[...], nt, preferred_element_type=jnp.float32),
        gains_ref[64:128, :], cosine, sine,
    )
    kv[me, 0:256, :] = jnp.concatenate(kt, axis=0).T.astype(jnp.bfloat16)
    vt = lax.dot_general(same, v_ref[...], nt, preferred_element_type=jnp.float32).astype(jnp.bfloat16)
    kv[me, 256:384, :] = vt[:, 0:128]
    kv[me, 384:512, :] = vt[:, 128:256]

    qt[...] = jnp.zeros_like(qt)
    for j in range(4):
        heads = turned_heads(
            lax.dot_general(
                order, q_ref[:, 128 * j : 128 * j + 128], nt, preferred_element_type=jnp.float32
            ),
            gains_ref[0:64, :], cosine, sine,
        )
        for i in range(2):
            scaled = heads[i].astype(jnp.bfloat16).astype(jnp.float32) * QSCALE
            high = scaled.astype(jnp.bfloat16)
            low = (scaled - high.astype(jnp.float32)).astype(jnp.bfloat16)
            at, to = pl.ds((2 * j + i) * 256, 256), 64 * (j // 2)
            qt[to : to + 64, at] = high
            qt[128 + to : 192 + to, at] = low

    pl.semaphore_wait(barrier, 6)

    def copy(src, peer, slot):
        return pltpu.make_async_remote_copy(
            src_ref=kv.at[src], dst_ref=kv.at[src],
            send_sem=send_sem.at[src, slot], recv_sem=recv_sem.at[src],
            device_id=(peer, core), device_id_type=MESH_ID,
        )

    def start(src, peer, slot):
        copy(src, peer, slot).start()

    def finish(src, peer, slot):
        copy(src, peer, slot).wait_send()

    def take(offset):
        src = source_of(offset, me)
        copy(src, me, 0).wait_recv()
        each_send(offset, me, start)

    each_send(jnp.int32(0), me, start)

    own = kv[me, 0:256, :]
    own = jnp.concatenate([own, own], axis=1)
    for t in range(4):
        at = pl.ds(t * 512, 512)
        s = jnp.dot(own, qt[:, at], preferred_element_type=jnp.float32)
        top[:, at] = jnp.broadcast_to(jnp.max(s, axis=0, keepdims=True), (8, 512))
    acc[...] = jnp.zeros_like(acc)
    ones = jnp.ones((16, 1024), jnp.bfloat16)
    for n in range(1, 3):
        take(jnp.int32(ORDER[n]))

    first, ahead = packed(0), packed(3)

    def group(g, carry):
        coming = lookup(ahead, g)
        for j in range(4):

            @pl.when(4 * g + 3 + j < 64)
            def _():
                take((coming // 64**j) % 64)

        now = lookup(first, g)
        srcs = [source_of((now // 64**j) % 64, me) for j in range(4)]
        for s in srcs:
            pltpu.make_async_copy(kv.at[s], kv_out.at[s], out_sem.at[s]).start()
        kk = jnp.concatenate([kv[s, 0:256, :] for s in srcs], axis=0)
        kk = jnp.concatenate([kk, kk], axis=1)
        vt = jnp.concatenate([kv[s, a : a + 128, :] for s in srcs for a in (256, 384)], axis=1)
        va = [jnp.concatenate([vt[64 * h : 64 * h + 64], ones], axis=0) for h in range(2)]
        for t in range(4):
            at = pl.ds(t * 512, 512)
            s = jnp.dot(kk, qt[:, at], preferred_element_type=jnp.float32)
            p = jnp.exp2(s - top[0:1, at]).astype(jnp.bfloat16)
            acc[:, at] += jnp.dot(va[t // 2], p, preferred_element_type=jnp.float32)
        return carry

    lax.fori_loop(0, 16, group, 0)

    for j in range(4):
        parts = []
        for i in range(2):
            at = pl.ds((2 * j + i) * 256, 256)
            parts.append(acc[0:64, at] / acc[64:65, at])
        o_ref[:, 128 * j : 128 * j + 128] = jnp.concatenate(parts, axis=0).T.astype(jnp.bfloat16)
    den_ref[...] = jnp.broadcast_to(jnp.max(acc[64:65, :]), (8, 128))

    def drain(g, carry):
        now = lookup(first, g)
        for j in range(4):
            offset = (now // 64**j) % 64
            each_send(offset, me, finish)
            s = source_of(offset, me)
            pltpu.make_async_copy(kv.at[s], kv_out.at[s], out_sem.at[s]).wait()
        return carry

    lax.fori_loop(0, 16, drain, 0)


def attention(queries, keys, values, q_gain, k_gain):
    me = lax.axis_index("sp")
    half = HEAD_DIM // 2
    freqs = THETA ** (-jnp.arange(0, half, 2, dtype=jnp.float32) / half)
    positions = me * 256 + jnp.arange(256, dtype=jnp.int32)
    grid_row = (positions // GRID_W).astype(jnp.float32)
    grid_col = (positions % GRID_W).astype(jnp.float32)
    angles = jnp.concatenate([freqs[:, None] * grid_row, freqs[:, None] * grid_col], axis=0)
    trig = jnp.concatenate([jnp.cos(angles), jnp.sin(angles)], axis=0)
    pairs = [g.reshape(32, 2).T.reshape(64) for g in (q_gain, k_gain)]
    gains = jnp.broadcast_to(jnp.concatenate(pairs)[:, None], (128, 256))
    vmem = pl.BlockSpec(memory_space=pltpu.VMEM)
    return pl.pallas_call(
        attention_kernel,
        out_shape=(
            jax.ShapeDtypeStruct((256, 512), jnp.bfloat16),
            jax.ShapeDtypeStruct((8, 128), jnp.float32),
            jax.ShapeDtypeStruct((64, 512, 128), jnp.bfloat16),
        ),
        in_specs=[vmem] * 5,
        out_specs=(vmem, vmem, pl.BlockSpec(memory_space=pltpu.HBM)),
        scratch_shapes=[
            pltpu.VMEM((256, 2048), jnp.bfloat16),
            pltpu.VMEM((8, 2048), jnp.float32),
            pltpu.VMEM((80, 2048), jnp.float32),
            pltpu.VMEM((64, 512, 128), jnp.bfloat16),
            pltpu.SemaphoreType.DMA((64, 6)),
            pltpu.SemaphoreType.DMA((64,)),
            pltpu.SemaphoreType.DMA((64,)),
        ],
        compiler_params=pltpu.CompilerParams(
            collective_id=0, has_side_effects=True, vmem_limit_bytes=56 << 20
        ),
        cost_estimate=pl.CostEstimate(flops=17_000_000_000, bytes_accessed=9_000_000, transcendentals=0),
        name="attention",
    )(queries, keys, values, gains, trig)


def attention_again(queries, q_gain, kv):
    me = lax.axis_index("sp")
    positions = me * 256 + jnp.arange(256, dtype=jnp.int32)
    qn = qk_prepare(queries, q_gain, positions, 8).reshape(256, 2, 4, 32, 2)
    qn = jnp.swapaxes(qn, -1, -2).reshape(256, 2, 4, 64)
    k = kv[:, 0:256].reshape(64, 256, 2, 64)
    v = jnp.concatenate([kv[:, 256:384], kv[:, 384:512]], axis=2).reshape(64, 2, 64, 256)

    def scores_of(kb):
        return jnp.einsum("qhgd,khd->hgqk", qn, kb, preferred_element_type=jnp.float32) * 0.125

    def largest(m, kb):
        return jnp.maximum(m, jnp.max(scores_of(kb), axis=-1)), None

    top, _ = lax.scan(largest, jnp.full((2, 4, 256), -1e30, jnp.float32), k)

    def add(carry, block):
        total, summed = carry
        kb, vb = block
        ex = jnp.exp(scores_of(kb) - top[..., None])
        summed += jnp.einsum(
            "hgqk,hdk->hgqd", ex.astype(jnp.bfloat16), vb, preferred_element_type=jnp.float32
        )
        return (total + jnp.sum(ex, axis=-1), summed), None

    zero = (jnp.zeros((2, 4, 256), jnp.float32), jnp.zeros((2, 4, 256, 64), jnp.float32))
    (total, summed), _ = lax.scan(add, zero, (k, v))
    out = jnp.transpose(summed / total[..., None], (2, 0, 1, 3))
    return out.reshape(256, 512).astype(jnp.bfloat16)


def per_device(
    queries,
    keys,
    values,
    q_gain,
    k_gain,
    resid,
    out_weight,
    post_gain,
    ffn_gain,
    post_ffn_gain,
    gate_w,
    up_w,
    down_w,
    route_ids,
    route_w,
):
    tok_local = queries.shape[0]
    width = resid.shape[1]
    tp_count = lax.axis_size("tp")
    sp_count = lax.axis_size("sp")
    attended, den, kv = attention(queries, keys, values, q_gain, k_gain)
    attended = lax.cond(
        den[0, 0] < LIMIT,
        lambda: attended,
        lambda: attention_again(queries, q_gain, kv),
    )
    row_count = tok_local // tp_count
    token_heads = lax.all_to_all(attended, "tp", split_axis=0, concat_axis=1, tiled=True)
    mixed = jnp.dot(
        token_heads,
        lax.all_gather(out_weight, "tp", axis=0, tiled=True),
        preferred_element_type=jnp.float32,
    )
    hidden_state = (resid.astype(jnp.float32) + rms_scale(mixed, post_gain)).astype(jnp.bfloat16)
    normed = rms_scale(hidden_state.astype(jnp.float32), ffn_gain).astype(jnp.bfloat16)
    top_count = route_ids.shape[1]
    expert_count = gate_w.shape[0] * sp_count
    capacity = 3 * tok_local * top_count // (2 * tp_count * expert_count)
    flat_routes = route_ids.reshape(-1)
    chosen = (flat_routes[:, None] == jnp.arange(expert_count, dtype=jnp.int32)[None, :]).astype(
        jnp.int32
    )
    earlier = jnp.cumsum(chosen, axis=0) - chosen
    ranks = jnp.sum(earlier * chosen, axis=1)
    slot_ids = flat_routes * capacity + ranks
    slot_range = jnp.arange(expert_count * capacity, dtype=jnp.int32)
    selector = jnp.sum(
        (slot_ids.reshape(row_count, top_count)[:, :, None] == slot_range[None, None, :]).astype(
            jnp.bfloat16
        ),
        axis=1,
    )
    outgoing = lax.dot_general(
        selector, normed, (((0,), (0,)), ((), ())), preferred_element_type=jnp.float32
    )
    outgoing = outgoing.astype(jnp.bfloat16).reshape(expert_count, capacity, width)
    arrived = lax.all_to_all(outgoing, "sp", split_axis=0, concat_axis=0, tiled=True)

    def expand(piece, start_row):
        flat_rows = piece.reshape(-1, width)
        gate = jnp.dot(flat_rows, gate_w[0], preferred_element_type=jnp.float32)
        upward = jnp.dot(flat_rows, up_w[0], preferred_element_type=jnp.float32)
        return (jax.nn.silu(gate) * upward).astype(jnp.bfloat16)

    inner = work_in_pieces(arrived, "tp", 0, expand, 0)
    expert_out = summed_on_arrival(
        jnp.dot(inner, down_w[0], preferred_element_type=jnp.float32).astype(jnp.bfloat16), "tp", 0
    ).astype(jnp.bfloat16)
    returned = lax.all_to_all(
        expert_out.reshape(expert_count, capacity, width),
        "sp",
        split_axis=0,
        concat_axis=0,
        tiled=True,
    )
    picked = returned.reshape(expert_count * capacity, width)[slot_ids]
    picked = picked.reshape(row_count, top_count, width).astype(jnp.float32)
    combined = jnp.sum(route_w[:, :, None] * picked, axis=1)
    return (hidden_state.astype(jnp.float32) + rms_scale(combined, post_ffn_gain)).astype(
        jnp.bfloat16
    )


def solution(mesh):
    in_specs = (
        P("sp", "tp"),
        P("sp", "tp"),
        P("sp", "tp"),
        P(),
        P(),
        P(("sp", "tp"), None),
        P("tp", None),
        P(),
        P(),
        P(),
        P("sp", None, "tp"),
        P("sp", None, "tp"),
        P("sp", "tp", None),
        P(("sp", "tp"), None),
        P(("sp", "tp"), None),
    )
    out_specs = P(("sp", "tp"), None)
    return jax.shard_map(
        per_device, mesh=mesh, in_specs=in_specs, out_specs=out_specs, check_vma=False
    )
```

```python
import jax
import jax.numpy as jnp
from jax import lax
from jax.experimental import pallas as pl
from jax.experimental.pallas import tpu as pltpu
from jax.sharding import PartitionSpec as P

HEAD_DIM = 64
GRID_W = 64


EPS = 1e-06
THETA = 10000.0


def qk_prepare(raw, gain, positions, head_count):
    count_rows = raw.shape[0]
    values32 = raw.astype(jnp.float32).reshape(count_rows, head_count, HEAD_DIM)
    normed = (
        values32 * lax.rsqrt(jnp.mean(values32 * values32, axis=-1, keepdims=True) + EPS) * gain
    )
    half_dim = HEAD_DIM // 2
    freqs = THETA ** (-jnp.arange(0, half_dim, 2, dtype=jnp.float32) / half_dim)
    grid_row = (positions // GRID_W).astype(jnp.float32)
    grid_col = (positions % GRID_W).astype(jnp.float32)
    angles = jnp.concatenate([grid_row[:, None] * freqs, grid_col[:, None] * freqs], axis=-1)
    cosine = jnp.cos(angles)[:, None, :]
    sine = jnp.sin(angles)[:, None, :]
    paired = normed.reshape(count_rows, head_count, half_dim, 2)
    first = paired[..., 0]
    second = paired[..., 1]
    turned = jnp.stack([first * cosine - second * sine, first * sine + second * cosine], axis=-1)
    return turned.reshape(count_rows, head_count * HEAD_DIM).astype(jnp.bfloat16)


def rms_scale(values32, gain):
    return values32 * lax.rsqrt(jnp.mean(values32 * values32, axis=-1, keepdims=True) + EPS) * gain


MESH_ID = pl.DeviceIdType.MESH
LIMIT = 2.0**100
QSCALE = 1.4426950408889634 / 8.0


def hops(d):
    return (0, 1, 2, 1)[d]


ORDER = sorted(range(64), key=lambda o: hops(o // 16) + hops(o // 4 % 4) + hops(o % 4))


def packed(start):
    words = []
    for g in range(16):
        w = 0
        for j in range(4):
            n = 4 * g + start + j
            w += (ORDER[n] if n < 64 else 0) * 64**j
        words.append(w)
    return words


def lookup(words, g):
    w = jnp.int32(words[0])
    for i in range(1, len(words)):
        w = jnp.where(g == i, jnp.int32(words[i]), w)
    return w


def pick(a, z, y, x):
    return jnp.where(a == 0, z, jnp.where(a == 1, y, x))


def source_of(offset, me):
    mz, my, mx = me // 16, (me // 4) % 4, me % 4
    cz = (mz + 4 - offset // 16) % 4
    cy = (my + 4 - (offset // 4) % 4) % 4
    cx = (mx + 4 - offset % 4) % 4
    return cz * 16 + cy * 4 + cx


def each_send(offset, me, act):
    mz, my, mx = me // 16, (me // 4) % 4, me % 4
    oz, oy, ox = offset // 16, (offset // 4) % 4, offset % 4
    src = source_of(offset, me)
    total = src // 16 + (src // 4) % 4 + src % 4
    kind, odd = total % 3, total % 2
    axes = [(kind + i) % 3 for i in range(3)]
    stride = [pick(a, 16, 4, 1) for a in axes]
    digit = [pick(a, oz, oy, ox) for a in axes]
    mine = [pick(a, mz, my, mx) for a in axes]

    def peer(i, step):
        return me + ((mine[i] + step) % 4 - mine[i]) * stride[i]

    none = offset == 0
    last = jnp.where(digit[2] > 0, 2, jnp.where(digit[1] > 0, 1, jnp.where(digit[0] > 0, 0, -1)))
    for i in range(3):

        @pl.when(i > last)
        def _():
            act(src, peer(i, 1), 2 * i)
            act(src, peer(i, 3), 2 * i + 1)

        @pl.when(jnp.logical_and(i == last, jnp.logical_and(digit[i] == 1, odd == 0)))
        def _():
            act(src, peer(i, 1), 2 * i)

        @pl.when(jnp.logical_and(i == last, jnp.logical_and(digit[i] == 3, odd == 1)))
        def _():
            act(src, peer(i, 3), 2 * i + 1)


def turned_heads(x, gain, cosine, sine):
    out = []
    for h in range(2):
        even, odd = x[64 * h : 64 * h + 32], x[64 * h + 32 : 64 * h + 64]
        squares = jnp.sum(even * even, axis=0, keepdims=True) + jnp.sum(odd * odd, axis=0, keepdims=True)
        scale = lax.rsqrt(squares * (1.0 / 64.0) + EPS)
        even, odd = even * scale * gain[0:32], odd * scale * gain[32:64]
        out.append(jnp.concatenate([even * cosine - odd * sine, even * sine + odd * cosine], axis=0))
    return out


def attention_kernel(
    q_ref, k_ref, v_ref, gains_ref, trig_ref, ow_ref, o_ref, den_ref, kv_out, ow_out,
    qt, top, acc, kv, send_sem, recv_sem, out_sem, swap_sem,
):
    me, core = lax.axis_index("sp"), lax.axis_index("tp")
    mz, my, mx = me // 16, (me // 4) % 4, me % 4
    barrier = pltpu.get_barrier_semaphore()
    for stride, c in ((16, mz), (4, my), (1, mx)):
        for step in (1, 3):
            to = me + ((c + step) % 4 - c) * stride
            pl.semaphore_signal(barrier, inc=1, device_id=(to, core), device_id_type=MESH_ID)
    pl.semaphore_signal(barrier, inc=1, device_id=(me, 1 - core), device_id_type=MESH_ID)

    row = lax.broadcasted_iota(jnp.int32, (128, 128), 0)
    col = lax.broadcasted_iota(jnp.int32, (128, 128), 1)
    within = row % 64
    wanted = (row // 64) * 64 + 2 * (within % 32) + within // 32
    order = (col == wanted).astype(jnp.float32).astype(jnp.bfloat16)
    same = (col == row).astype(jnp.float32).astype(jnp.bfloat16)
    nt = (((1,), (1,)), ((), ()))
    cosine, sine = trig_ref[0:32, :], trig_ref[32:64, :]
    kt = turned_heads(
        lax.dot_general(order, k_ref[...], nt, preferred_element_type=jnp.float32),
        gains_ref[64:128, :], cosine, sine,
    )
    kv[me, 0:256, :] = jnp.concatenate(kt, axis=0).T.astype(jnp.bfloat16)
    vt = lax.dot_general(same, v_ref[...], nt, preferred_element_type=jnp.float32).astype(jnp.bfloat16)
    kv[me, 256:384, :] = vt[:, 0:128]
    kv[me, 384:512, :] = vt[:, 128:256]

    qt[...] = jnp.zeros_like(qt)
    for j in range(4):
        heads = turned_heads(
            lax.dot_general(
                order, q_ref[:, 128 * j : 128 * j + 128], nt, preferred_element_type=jnp.float32
            ),
            gains_ref[0:64, :], cosine, sine,
        )
        for i in range(2):
            scaled = heads[i].astype(jnp.bfloat16).astype(jnp.float32) * QSCALE
            high = scaled.astype(jnp.bfloat16)
            low = (scaled - high.astype(jnp.float32)).astype(jnp.bfloat16)
            at, to = pl.ds((2 * j + i) * 256, 256), 64 * (j // 2)
            qt[to : to + 64, at] = high
            qt[128 + to : 192 + to, at] = low

    pl.semaphore_wait(barrier, 7)

    def copy(src, peer, slot):
        return pltpu.make_async_remote_copy(
            src_ref=kv.at[src], dst_ref=kv.at[src],
            send_sem=send_sem.at[src, slot], recv_sem=recv_sem.at[src],
            device_id=(peer, core), device_id_type=MESH_ID,
        )

    def start(src, peer, slot):
        copy(src, peer, slot).start()

    def finish(src, peer, slot):
        copy(src, peer, slot).wait_send()

    def take(offset):
        src = source_of(offset, me)
        copy(src, me, 0).wait_recv()
        each_send(offset, me, start)

    each_send(jnp.int32(0), me, start)
    swap = pltpu.make_async_remote_copy(
        src_ref=ow_ref, dst_ref=ow_out, send_sem=swap_sem.at[0], recv_sem=swap_sem.at[1],
        device_id=(me, 1 - core), device_id_type=MESH_ID,
    )
    swap.start()

    own = kv[me, 0:256, :]
    own = jnp.concatenate([own, own], axis=1)
    for t in range(4):
        at = pl.ds(t * 512, 512)
        s = jnp.dot(own, qt[:, at], preferred_element_type=jnp.float32)
        top[:, at] = jnp.broadcast_to(jnp.max(s, axis=0, keepdims=True), (8, 512))
    acc[...] = jnp.zeros_like(acc)
    ones = jnp.ones((16, 1024), jnp.bfloat16)
    for n in range(1, 3):
        take(jnp.int32(ORDER[n]))

    first, ahead = packed(0), packed(3)

    def group(g, carry):
        coming = lookup(ahead, g)
        for j in range(4):

            @pl.when(4 * g + 3 + j < 64)
            def _():
                take((coming // 64**j) % 64)

        now = lookup(first, g)
        srcs = [source_of((now // 64**j) % 64, me) for j in range(4)]
        for s in srcs:
            pltpu.make_async_copy(kv.at[s], kv_out.at[s], out_sem.at[s]).start()
        kk = jnp.concatenate([kv[s, 0:256, :] for s in srcs], axis=0)
        kk = jnp.concatenate([kk, kk], axis=1)
        vt = jnp.concatenate([kv[s, a : a + 128, :] for s in srcs for a in (256, 384)], axis=1)
        va = [jnp.concatenate([vt[64 * h : 64 * h + 64], ones], axis=0) for h in range(2)]
        for t in range(4):
            at = pl.ds(t * 512, 512)
            s = jnp.dot(kk, qt[:, at], preferred_element_type=jnp.float32)
            p = jnp.exp2(s - top[0:1, at]).astype(jnp.bfloat16)
            acc[:, at] += jnp.dot(va[t // 2], p, preferred_element_type=jnp.float32)
        return carry

    lax.fori_loop(0, 16, group, 0)

    for j in range(4):
        parts = []
        for i in range(2):
            at = pl.ds((2 * j + i) * 256, 256)
            parts.append(acc[0:64, at] / acc[64:65, at])
        o_ref[:, 128 * j : 128 * j + 128] = jnp.concatenate(parts, axis=0).T.astype(jnp.bfloat16)
    den_ref[...] = jnp.broadcast_to(jnp.max(acc[64:65, :]), (8, 128))

    def drain(g, carry):
        now = lookup(first, g)
        for j in range(4):
            offset = (now // 64**j) % 64
            each_send(offset, me, finish)
            s = source_of(offset, me)
            pltpu.make_async_copy(kv.at[s], kv_out.at[s], out_sem.at[s]).wait()
        return carry

    lax.fori_loop(0, 16, drain, 0)
    swap.wait()


def attention(queries, keys, values, q_gain, k_gain, out_weight):
    me = lax.axis_index("sp")
    half = HEAD_DIM // 2
    freqs = THETA ** (-jnp.arange(0, half, 2, dtype=jnp.float32) / half)
    positions = me * 256 + jnp.arange(256, dtype=jnp.int32)
    grid_row = (positions // GRID_W).astype(jnp.float32)
    grid_col = (positions % GRID_W).astype(jnp.float32)
    angles = jnp.concatenate([freqs[:, None] * grid_row, freqs[:, None] * grid_col], axis=0)
    trig = jnp.concatenate([jnp.cos(angles), jnp.sin(angles)], axis=0)
    pairs = [g.reshape(32, 2).T.reshape(64) for g in (q_gain, k_gain)]
    gains = jnp.broadcast_to(jnp.concatenate(pairs)[:, None], (128, 256))
    vmem, hbm = pl.BlockSpec(memory_space=pltpu.VMEM), pl.BlockSpec(memory_space=pltpu.HBM)
    return pl.pallas_call(
        attention_kernel,
        out_shape=(
            jax.ShapeDtypeStruct((256, 512), jnp.bfloat16),
            jax.ShapeDtypeStruct((8, 128), jnp.float32),
            jax.ShapeDtypeStruct((64, 512, 128), jnp.bfloat16),
            jax.ShapeDtypeStruct((512, 2048), jnp.bfloat16),
        ),
        in_specs=[vmem] * 5 + [hbm],
        out_specs=(vmem, vmem, hbm, hbm),
        scratch_shapes=[
            pltpu.VMEM((256, 2048), jnp.bfloat16),
            pltpu.VMEM((8, 2048), jnp.float32),
            pltpu.VMEM((80, 2048), jnp.float32),
            pltpu.VMEM((64, 512, 128), jnp.bfloat16),
            pltpu.SemaphoreType.DMA((64, 6)),
            pltpu.SemaphoreType.DMA((64,)),
            pltpu.SemaphoreType.DMA((64,)),
            pltpu.SemaphoreType.DMA((2,)),
        ],
        compiler_params=pltpu.CompilerParams(
            collective_id=0, has_side_effects=True, vmem_limit_bytes=56 << 20
        ),
        cost_estimate=pl.CostEstimate(flops=17_000_000_000, bytes_accessed=9_000_000, transcendentals=0),
        name="attention",
    )(queries, keys, values, gains, trig, out_weight)


def attention_again(queries, q_gain, kv):
    me = lax.axis_index("sp")
    positions = me * 256 + jnp.arange(256, dtype=jnp.int32)
    qn = qk_prepare(queries, q_gain, positions, 8).reshape(256, 2, 4, 32, 2)
    qn = jnp.swapaxes(qn, -1, -2).reshape(256, 2, 4, 64)
    k = kv[:, 0:256].reshape(64, 256, 2, 64)
    v = jnp.concatenate([kv[:, 256:384], kv[:, 384:512]], axis=2).reshape(64, 2, 64, 256)

    def scores_of(kb):
        return jnp.einsum("qhgd,khd->hgqk", qn, kb, preferred_element_type=jnp.float32) * 0.125

    def largest(m, kb):
        return jnp.maximum(m, jnp.max(scores_of(kb), axis=-1)), None

    top, _ = lax.scan(largest, jnp.full((2, 4, 256), -1e30, jnp.float32), k)

    def add(carry, block):
        total, summed = carry
        kb, vb = block
        ex = jnp.exp(scores_of(kb) - top[..., None])
        summed += jnp.einsum(
            "hgqk,hdk->hgqd", ex.astype(jnp.bfloat16), vb, preferred_element_type=jnp.float32
        )
        return (total + jnp.sum(ex, axis=-1), summed), None

    zero = (jnp.zeros((2, 4, 256), jnp.float32), jnp.zeros((2, 4, 256, 64), jnp.float32))
    (total, summed), _ = lax.scan(add, zero, (k, v))
    out = jnp.transpose(summed / total[..., None], (2, 0, 1, 3))
    return out.reshape(256, 512).astype(jnp.bfloat16)


SLOTS = 6
PLANE = 16 * SLOTS


def experts_kernel(
    att_ref, resid_ref, gains_ref, ids_ref, rw_ref, ow_ref, owp_ref, gate_hbm, up_hbm, down_hbm, o_ref,
    ow, owp, gate, up, down, att_in, hidden, out, arr, x, inner, part, part_out, part_in, total, ret, combined, tiles,
    w_sem, a_sem, d_send, d_recv, f_send, f_recv, p_send, p_recv, r_send, r_recv,
):
    me, core = lax.axis_index("sp"), lax.axis_index("tp")
    mz, mq = me // 16, me % 16
    other = 1 - core
    f32, bf16 = jnp.float32, jnp.bfloat16

    barrier = pltpu.get_barrier_semaphore()

    def greet(i, carry):
        pl.semaphore_signal(barrier, inc=1, device_id=((me + i) % 64, core), device_id_type=MESH_ID)
        return carry

    lax.fori_loop(1, 64, greet, 0)
    pl.semaphore_signal(barrier, inc=1, device_id=(me, other), device_id_type=MESH_ID)
    loads = [
        pltpu.make_async_copy(src, dst, w_sem.at[i])
        for i, (src, dst) in enumerate(
            ((ow_ref, ow), (owp_ref, owp), (gate_hbm.at[0], gate), (up_hbm.at[0], up), (down_hbm.at[0], down))
        )
    ]
    for load in loads:
        load.start()

    lane = lax.broadcasted_iota(jnp.int32, (128, 64), 1)
    chosen = [(ids_ref[:, k : k + 1] == lane).astype(f32) for k in range(2)]
    below = (
        lax.broadcasted_iota(jnp.int32, (128, 128), 1) < lax.broadcasted_iota(jnp.int32, (128, 128), 0)
    ).astype(f32).astype(bf16)
    earlier = [jnp.dot(below, c.astype(bf16), preferred_element_type=f32) for c in chosen]
    earlier[1] = earlier[1] + jnp.sum(chosen[0], axis=0, keepdims=True)
    slot = [
        ids_ref[:, k : k + 1] * SLOTS
        + jnp.sum(earlier[k] * chosen[k], axis=1, keepdims=True).astype(jnp.int32)
        for k in range(2)
    ]
    within = lax.broadcasted_iota(jnp.int32, (128, PLANE), 1)

    def offset_of(j):
        return jnp.where(j == 2, 3, jnp.where(j == 3, 2, j))

    pl.semaphore_wait(barrier, 64)

    here = pl.ds(pl.multiple_of(core * 128, 128), 128)
    there = pl.ds(pl.multiple_of(other * 128, 128), 128)
    swap = pltpu.make_async_remote_copy(
        src_ref=att_ref.at[there], dst_ref=att_in, send_sem=a_sem.at[0], recv_sem=a_sem.at[1],
        device_id=(me, other), device_id_type=MESH_ID,
    )
    swap.start()
    loads[0].wait()
    mixed = jnp.dot(att_ref[here, :], ow[...], preferred_element_type=f32)
    loads[1].wait()
    swap.wait()
    mixed = mixed + jnp.dot(att_in[...], owp[...], preferred_element_type=f32)
    state = (resid_ref[...].astype(f32) + rms_scale(mixed, gains_ref[0:1, :])).astype(bf16)
    hidden[...] = state
    normed = rms_scale(state.astype(f32), gains_ref[1:2, :]).astype(bf16)

    def block(ref, s):
        return ref.at[pl.ds(s * SLOTS, SLOTS)]

    def there_copy(s):
        return pltpu.make_async_remote_copy(
            src_ref=block(out, s), dst_ref=block(arr.at[core], me), send_sem=d_send.at[s], recv_sem=d_recv.at[me],
            device_id=(s, core), device_id_type=MESH_ID,
        )

    def arrival(s):
        return pltpu.make_async_remote_copy(
            src_ref=block(out, s), dst_ref=block(arr.at[core], s), send_sem=d_send.at[s], recv_sem=d_recv.at[s],
            device_id=(s, core), device_id_type=MESH_ID,
        )

    def back_copy(s):
        return pltpu.make_async_remote_copy(
            src_ref=block(total, s), dst_ref=block(ret, me), send_sem=r_send.at[s], recv_sem=r_recv.at[me],
            device_id=(s, core), device_id_type=MESH_ID,
        )

    def back_arrival(s):
        return pltpu.make_async_remote_copy(
            src_ref=block(total, s), dst_ref=block(ret, s), send_sem=r_send.at[s], recv_sem=r_recv.at[s],
            device_id=(s, core), device_id_type=MESH_ID,
        )

    def for_plane(z, first, act):
        def step(i, carry):
            act(z * 16 + (mq + i) % 16)
            return carry

        lax.fori_loop(first, 16, step, 0)

    def skip(j):
        return jnp.where(j == 0, 1, 0)

    def dispatch(j, carry):
        z = (mz + offset_of(j)) % 4
        place = within + z * PLANE
        picked = ((slot[0] == place).astype(f32) + (slot[1] == place).astype(f32)).astype(bf16)
        rows = lax.dot_general(picked, normed, (((0,), (0,)), ((), ())), preferred_element_type=f32)
        tiles[...] = rows.astype(bf16).reshape(PLANE, 16, 128)
        out[pl.ds(z * PLANE, PLANE)] = tiles[...]
        for_plane(z, skip(j), lambda s: there_copy(s).start())
        return carry

    lax.fori_loop(0, 4, dispatch, 0)
    arr[core, pl.ds(me * SLOTS, SLOTS)] = out[pl.ds(me * SLOTS, SLOTS)]
    for load in loads[2:]:
        load.wait()

    def forward(j):
        z = (mz + 4 - offset_of(j)) % 4
        rows = pl.ds(z * PLANE, PLANE)
        return pltpu.make_async_remote_copy(
            src_ref=arr.at[core, rows], dst_ref=arr.at[core, rows], send_sem=f_send.at[j], recv_sem=f_recv.at[j],
            device_id=(me, other), device_id_type=MESH_ID,
        )

    def partial(j):
        return pltpu.make_async_remote_copy(
            src_ref=part_out.at[j], dst_ref=part_in.at[j], send_sem=p_send.at[j], recv_sem=p_recv.at[j],
            device_id=(me, other), device_id_type=MESH_ID,
        )

    def finish(j):
        z = (mz + 4 - offset_of(j)) % 4
        partial(j).wait_recv()
        rows = (part[j].astype(f32) + part_in[j].astype(f32)).astype(bf16)
        tiles[...] = rows.reshape(PLANE, 16, 128)
        total[pl.ds(z * PLANE, PLANE)] = tiles[...]

        @pl.when(j == 0)
        def _():
            ret[pl.ds(me * SLOTS, SLOTS)] = total[pl.ds(me * SLOTS, SLOTS)]

        for_plane(z, skip(j), lambda s: back_copy(s).start())

    def chunk(j, carry):
        z = (mz + 4 - offset_of(j)) % 4
        rows = pl.ds(z * PLANE, PLANE)
        for_plane(z, skip(j), lambda s: arrival(s).wait_recv())
        forward(j).start()
        tiles[...] = arr[core, rows]
        x[0:PLANE, :] = tiles[...].reshape(PLANE, 2048)
        forward(j).wait_recv()
        tiles[...] = arr[other, rows]
        x[PLANE : 2 * PLANE, :] = tiles[...].reshape(PLANE, 2048)
        for n in range(7):
            at = pl.ds(n * 256, 256)
            g = jnp.dot(x[...], gate[:, at], preferred_element_type=f32)
            u = jnp.dot(x[...], up[:, at], preferred_element_type=f32)
            inner[:, at] = (g / (1.0 + jnp.exp(-g)) * u).astype(bf16)
        for n in range(8):
            at = pl.ds(n * 256, 256)
            y = jnp.dot(inner[...], down[:, at], preferred_element_type=f32).astype(bf16)
            part[j, :, at] = y[0:PLANE]
            part_out[j, :, at] = y[PLANE : 2 * PLANE]

        partial(j).start()

        @pl.when(j > 0)
        def _():
            finish(j - 1)

        return carry

    lax.fori_loop(0, 4, chunk, 0)
    finish(jnp.int32(3))

    combined[...] = jnp.zeros_like(combined)

    def collect(j, carry):
        z = (mz + offset_of(j)) % 4
        for_plane(z, skip(j), lambda s: back_arrival(s).wait_recv())
        place = within + z * PLANE
        weight = jnp.where(slot[0] == place, rw_ref[:, 0:1], 0.0) + jnp.where(slot[1] == place, rw_ref[:, 1:2], 0.0)
        high = weight.astype(bf16)
        low = (weight - high.astype(f32)).astype(bf16)
        tiles[...] = ret[pl.ds(z * PLANE, PLANE)]
        rows = tiles[...].reshape(PLANE, 2048)
        combined[...] += jnp.dot(high, rows, preferred_element_type=f32) + jnp.dot(
            low, rows, preferred_element_type=f32
        )
        return carry

    lax.fori_loop(0, 4, collect, 0)
    o_ref[...] = (hidden[...].astype(f32) + rms_scale(combined[...], gains_ref[2:3, :])).astype(bf16)

    swap_sends = [forward, partial]

    def drain(j, carry):
        for_plane(j, jnp.where(j == mz, 1, 0), lambda s: there_copy(s).wait_send())
        for_plane(j, jnp.where(j == mz, 1, 0), lambda s: back_copy(s).wait_send())
        for make in swap_sends:
            make(j).wait_send()
        return carry

    lax.fori_loop(0, 4, drain, 0)


def experts(attended, resid, gains, route_ids, route_w, out_weight, out_weight_other, gate_w, up_w, down_w):
    vmem, hbm = pl.BlockSpec(memory_space=pltpu.VMEM), pl.BlockSpec(memory_space=pltpu.HBM)
    bf16, f32, dma = jnp.bfloat16, jnp.float32, pltpu.SemaphoreType.DMA
    return pl.pallas_call(
        experts_kernel,
        out_shape=jax.ShapeDtypeStruct((128, 2048), bf16),
        in_specs=[vmem] * 5 + [hbm] * 5,
        out_specs=vmem,
        scratch_shapes=[
            pltpu.VMEM((512, 2048), bf16),
            pltpu.VMEM((512, 2048), bf16),
            pltpu.VMEM((2048, 1792), bf16),
            pltpu.VMEM((2048, 1792), bf16),
            pltpu.VMEM((1792, 2048), bf16),
            pltpu.VMEM((128, 512), bf16),
            pltpu.VMEM((128, 2048), bf16),
            pltpu.VMEM((384, 16, 128), bf16),
            pltpu.VMEM((2, 384, 16, 128), bf16),
            pltpu.VMEM((2 * PLANE, 2048), bf16),
            pltpu.VMEM((2 * PLANE, 1792), bf16),
            pltpu.VMEM((4, PLANE, 2048), bf16),
            pltpu.VMEM((4, PLANE, 2048), bf16),
            pltpu.VMEM((4, PLANE, 2048), bf16),
            pltpu.VMEM((384, 16, 128), bf16),
            pltpu.VMEM((384, 16, 128), bf16),
            pltpu.VMEM((128, 2048), f32),
            pltpu.VMEM((PLANE, 16, 128), bf16),
            dma((5,)), dma((2,)), dma((64,)), dma((64,)), dma((4,)), dma((4,)), dma((4,)), dma((4,)),
            dma((64,)), dma((64,)),
        ],
        compiler_params=pltpu.CompilerParams(
            collective_id=1, has_side_effects=True, vmem_limit_bytes=60 << 20
        ),
        cost_estimate=pl.CostEstimate(flops=20_000_000_000, bytes_accessed=28_000_000, transcendentals=0),
        name="experts",
    )(attended, resid, gains, route_ids, route_w, out_weight, out_weight_other, gate_w, up_w, down_w)


def per_device(
    queries,
    keys,
    values,
    q_gain,
    k_gain,
    resid,
    out_weight,
    post_gain,
    ffn_gain,
    post_ffn_gain,
    gate_w,
    up_w,
    down_w,
    route_ids,
    route_w,
):
    attended, den, kv, out_weight_other = attention(queries, keys, values, q_gain, k_gain, out_weight)
    attended = lax.cond(
        den[0, 0] < LIMIT,
        lambda: attended,
        lambda: attention_again(queries, q_gain, kv),
    )
    gains = jnp.concatenate([post_gain[None], ffn_gain[None], post_ffn_gain[None], jnp.zeros((5, 2048), jnp.float32)])
    return experts(
        attended, resid, gains, route_ids, route_w, out_weight, out_weight_other, gate_w, up_w, down_w
    )


def solution(mesh):
    in_specs = (
        P("sp", "tp"),
        P("sp", "tp"),
        P("sp", "tp"),
        P(),
        P(),
        P(("sp", "tp"), None),
        P("tp", None),
        P(),
        P(),
        P(),
        P("sp", None, "tp"),
        P("sp", None, "tp"),
        P("sp", "tp", None),
        P(("sp", "tp"), None),
        P(("sp", "tp"), None),
    )
    out_specs = P(("sp", "tp"), None)
    return jax.shard_map(
        per_device, mesh=mesh, in_specs=in_specs, out_specs=out_specs, check_vma=False
    )
```

```python
import jax
import jax.numpy as jnp
from jax import lax
from jax.experimental import pallas as pl
from jax.experimental.pallas import tpu as pltpu
from jax.sharding import PartitionSpec as P

HEAD_DIM = 64
GRID_W = 64


EPS = 1e-06
THETA = 10000.0


def qk_prepare(raw, gain, positions, head_count):
    count_rows = raw.shape[0]
    values32 = raw.astype(jnp.float32).reshape(count_rows, head_count, HEAD_DIM)
    normed = (
        values32 * lax.rsqrt(jnp.mean(values32 * values32, axis=-1, keepdims=True) + EPS) * gain
    )
    half_dim = HEAD_DIM // 2
    freqs = THETA ** (-jnp.arange(0, half_dim, 2, dtype=jnp.float32) / half_dim)
    grid_row = (positions // GRID_W).astype(jnp.float32)
    grid_col = (positions % GRID_W).astype(jnp.float32)
    angles = jnp.concatenate([grid_row[:, None] * freqs, grid_col[:, None] * freqs], axis=-1)
    cosine = jnp.cos(angles)[:, None, :]
    sine = jnp.sin(angles)[:, None, :]
    paired = normed.reshape(count_rows, head_count, half_dim, 2)
    first = paired[..., 0]
    second = paired[..., 1]
    turned = jnp.stack([first * cosine - second * sine, first * sine + second * cosine], axis=-1)
    return turned.reshape(count_rows, head_count * HEAD_DIM).astype(jnp.bfloat16)


def rms_scale(values32, gain):
    return values32 * lax.rsqrt(jnp.mean(values32 * values32, axis=-1, keepdims=True) + EPS) * gain


MESH_ID = pl.DeviceIdType.MESH
LIMIT = 2.0**100
QSCALE = 1.4426950408889634 / 8.0
ORDER = [0, 12, 48, 4, 16, 3, 1, 60, 28, 8, 52, 15, 32, 19, 2, 51, 5, 7, 20, 17, 13, 49, 56, 11, 24, 18, 35, 21, 6, 29, 36, 50, 55, 44, 23, 9, 33, 14, 61, 63, 25, 53, 59, 39, 45, 40, 10, 62, 34, 22, 27, 47, 41, 58, 57, 30, 38, 54, 43, 37, 31, 26, 46, 42]
PARTS = ((0, 176), (176, 176), (352, 160))


def digits(offset):
    return (offset // 16, offset // 4 % 4, offset % 4)


def onward(offset, part):
    place = digits(offset)
    axes = [(part + i) % 3 for i in range(3)]
    last = max([i for i in range(3) if place[axes[i]]], default=-1)
    out = []
    if last >= 0:
        came = place[axes[last]]
        if came == (1, 3)[(sum(place) - came + part) % 2]:
            out.append((axes[last], came))
    for axis in axes[last + 1 :]:
        out += [(axis, 1), (axis, 3)]
    return out


def relay_plan():
    plan = [[(o, r) for r in range(3) for o in ORDER[1:7]]]
    for g in range(1, 16):
        plan.append([(o, r) for o in ORDER[4 * g + 3 : 4 * g + 7] for r in range(3)])
    return plan


def packed():
    return [sum(ORDER[4 * g + j] * 64**j for j in range(4)) for g in range(16)]


def lookup(words, g):
    w = jnp.int32(words[0])
    for i in range(1, len(words)):
        w = jnp.where(g == i, jnp.int32(words[i]), w)
    return w


def source_of(offset, me):
    cz = (me // 16 + 4 - offset // 16) % 4
    cy = ((me // 4) % 4 + 4 - (offset // 4) % 4) % 4
    cx = (me % 4 + 4 - offset % 4) % 4
    return cz * 16 + cy * 4 + cx


def turned_heads(x, gain, cosine, sine):
    out = []
    for h in range(2):
        even, odd = x[64 * h : 64 * h + 32], x[64 * h + 32 : 64 * h + 64]
        squares = jnp.sum(even * even, axis=0, keepdims=True) + jnp.sum(odd * odd, axis=0, keepdims=True)
        scale = lax.rsqrt(squares * (1.0 / 64.0) + EPS)
        even, odd = even * scale * gain[0:32], odd * scale * gain[32:64]
        out.append(jnp.concatenate([even * cosine - odd * sine, even * sine + odd * cosine], axis=0))
    return out


def attention_kernel(
    q_ref, k_ref, v_ref, qg_ref, kg_ref, ow_ref, o_ref, den_ref, kv_out, ow_out,
    qt, top, acc, kv, send_sem, recv_sem, out_sem, swap_sem,
):
    me, core = lax.axis_index("sp"), lax.axis_index("tp")
    coords = (me // 16, (me // 4) % 4, me % 4)
    peers = {
        (axis, step): me + ((coords[axis] + step) % 4 - coords[axis]) * (16, 4, 1)[axis]
        for axis in range(3)
        for step in (1, 3)
    }
    barrier = pltpu.get_barrier_semaphore()
    for to in peers.values():
        pl.semaphore_signal(barrier, inc=1, device_id=(to, core), device_id_type=MESH_ID)
    pl.semaphore_signal(barrier, inc=1, device_id=(me, 1 - core), device_id_type=MESH_ID)

    row = lax.broadcasted_iota(jnp.int32, (128, 128), 0)
    col = lax.broadcasted_iota(jnp.int32, (128, 128), 1)
    within = row % 64
    wanted = (row // 64) * 64 + 2 * (within % 32) + within // 32
    order = (col == wanted).astype(jnp.float32).astype(jnp.bfloat16)
    same = (col == row).astype(jnp.float32).astype(jnp.bfloat16)
    nt = (((1,), (1,)), ((), ()))

    pair = lax.broadcasted_iota(jnp.int32, (32, 256), 0)
    token = lax.broadcasted_iota(jnp.int32, (32, 256), 1)
    freq = jnp.zeros((32, 256), jnp.float32)
    for i in range(16):
        freq = jnp.where(pair % 16 == i, jnp.float32(THETA ** (-i / 16.0)), freq)
    where = jnp.where(pair < 16, me * 4 + token // 64, token % 64)
    angle = where.astype(jnp.float32) * freq
    cosine, sine = jnp.cos(angle), jnp.sin(angle)

    def column(ref):
        return jnp.sum(jnp.where((col == wanted)[0:64, 0:64], ref[...], 0.0), axis=1, keepdims=True)

    kt = turned_heads(
        lax.dot_general(order, k_ref[...], nt, preferred_element_type=jnp.float32), column(kg_ref), cosine, sine
    )
    kv[me, 0:256, :] = jnp.concatenate(kt, axis=0).T.astype(jnp.bfloat16)
    vt = lax.dot_general(same, v_ref[...], nt, preferred_element_type=jnp.float32).astype(jnp.bfloat16)
    kv[me, 256:384, :] = vt[:, 0:128]
    kv[me, 384:512, :] = vt[:, 128:256]

    pl.semaphore_wait(barrier, 7)

    sends = [0, 0, 0]

    def copy(src, part, to, number):
        rows = pl.ds(*PARTS[part])
        return pltpu.make_async_remote_copy(
            src_ref=kv.at[src, rows], dst_ref=kv.at[src, rows],
            send_sem=send_sem.at[part, number], recv_sem=recv_sem.at[part, src],
            device_id=(to, core), device_id_type=MESH_ID,
        )

    def pass_on(src, offset, part):
        for way in onward(offset, part):
            copy(src, part, peers[way], sends[part]).start()
            sends[part] += 1

    for part in range(3):
        pass_on(me, 0, part)
    swap = pltpu.make_async_remote_copy(
        src_ref=ow_ref, dst_ref=ow_out, send_sem=swap_sem.at[0], recv_sem=swap_sem.at[1],
        device_id=(me, 1 - core), device_id_type=MESH_ID,
    )

    qt[...] = jnp.zeros_like(qt)
    q_gain = column(qg_ref)
    for j in range(4):
        heads = turned_heads(
            lax.dot_general(
                order, q_ref[:, 128 * j : 128 * j + 128], nt, preferred_element_type=jnp.float32
            ),
            q_gain, cosine, sine,
        )
        for i in range(2):
            scaled = heads[i].astype(jnp.bfloat16).astype(jnp.float32) * QSCALE
            high = scaled.astype(jnp.bfloat16)
            low = (scaled - high.astype(jnp.float32)).astype(jnp.bfloat16)
            at, to = pl.ds((2 * j + i) * 256, 256), 64 * (j // 2)
            qt[to : to + 64, at] = high
            qt[128 + to : 192 + to, at] = low

    own = kv[me, 0:256, :]
    own = jnp.concatenate([own, own], axis=1)
    for t in range(4):
        at = pl.ds(t * 512, 512)
        s = jnp.dot(own, qt[:, at], preferred_element_type=jnp.float32)
        top[:, at] = jnp.broadcast_to(jnp.max(s, axis=0, keepdims=True), (8, 512))
    acc[...] = jnp.zeros_like(acc)
    ones = jnp.ones((16, 1024), jnp.bfloat16)

    words = packed()
    plan = relay_plan()

    def group(g, carry):
        for i, pieces in enumerate(plan):

            @pl.when(g == i)
            def _():
                for offset, part in pieces:
                    src = source_of(offset, me)
                    copy(src, part, me, 0).wait_recv()
                    pass_on(src, offset, part)
                if i == 1:
                    swap.start()

        now = lookup(words, g)
        srcs = [source_of((now // 64**j) % 64, me) for j in range(4)]
        for s in srcs:
            pltpu.make_async_copy(kv.at[s], kv_out.at[s], out_sem.at[s]).start()
        kk = jnp.concatenate([kv[s, 0:256, :] for s in srcs], axis=0)
        kk = jnp.concatenate([kk, kk], axis=1)
        vt = jnp.concatenate([kv[s, a : a + 128, :] for s in srcs for a in (256, 384)], axis=1)
        va = [jnp.concatenate([vt[64 * h : 64 * h + 64], ones], axis=0) for h in range(2)]
        for t in range(4):
            at = pl.ds(t * 512, 512)
            s = jnp.dot(kk, qt[:, at], preferred_element_type=jnp.float32)
            p = jnp.exp2(s - top[0:1, at]).astype(jnp.bfloat16)
            acc[:, at] += jnp.dot(va[t // 2], p, preferred_element_type=jnp.float32)
        return carry

    lax.fori_loop(0, 16, group, 0)

    for j in range(4):
        parts = []
        for i in range(2):
            at = pl.ds((2 * j + i) * 256, 256)
            parts.append(acc[0:64, at] / acc[64:65, at])
        o_ref[:, 128 * j : 128 * j + 128] = jnp.concatenate(parts, axis=0).T.astype(jnp.bfloat16)
    den_ref[0, 0] = jnp.max(acc[64:65, :])

    def drain(n, carry):
        for part in range(3):
            copy(me, part, me, n).wait_send()
        return carry

    def put_out(s, carry):
        pltpu.make_async_copy(kv.at[s], kv_out.at[s], out_sem.at[s]).wait()
        return carry

    lax.fori_loop(0, 63, drain, 0)
    lax.fori_loop(0, 64, put_out, 0)
    swap.wait()


def attention(queries, keys, values, q_gain, k_gain, out_weight):
    vmem, hbm = pl.BlockSpec(memory_space=pltpu.VMEM), pl.BlockSpec(memory_space=pltpu.HBM)
    return pl.pallas_call(
        attention_kernel,
        out_shape=(
            jax.ShapeDtypeStruct((256, 512), jnp.bfloat16),
            jax.ShapeDtypeStruct((1, 1), jnp.float32),
            jax.ShapeDtypeStruct((64, 512, 128), jnp.bfloat16),
            jax.ShapeDtypeStruct((512, 2048), jnp.bfloat16),
        ),
        in_specs=[vmem] * 5 + [hbm],
        out_specs=(vmem, pl.BlockSpec(memory_space=pltpu.SMEM), hbm, hbm),
        scratch_shapes=[
            pltpu.VMEM((256, 2048), jnp.bfloat16),
            pltpu.VMEM((8, 2048), jnp.float32),
            pltpu.VMEM((80, 2048), jnp.float32),
            pltpu.VMEM((64, 512, 128), jnp.bfloat16),
            pltpu.SemaphoreType.DMA((3, 63)),
            pltpu.SemaphoreType.DMA((3, 64)),
            pltpu.SemaphoreType.DMA((64,)),
            pltpu.SemaphoreType.DMA((2,)),
        ],
        compiler_params=pltpu.CompilerParams(
            collective_id=0, has_side_effects=True, vmem_limit_bytes=56 << 20
        ),
        cost_estimate=pl.CostEstimate(flops=17_000_000_000, bytes_accessed=9_000_000, transcendentals=0),
        name="attention",
    )(queries, keys, values, q_gain[None], k_gain[None], out_weight)


def attention_again(queries, q_gain, kv):
    me = lax.axis_index("sp")
    positions = me * 256 + jnp.arange(256, dtype=jnp.int32)
    qn = qk_prepare(queries, q_gain, positions, 8).reshape(256, 2, 4, 32, 2)
    qn = jnp.swapaxes(qn, -1, -2).reshape(256, 2, 4, 64)
    k = kv[:, 0:256].reshape(64, 256, 2, 64)
    v = jnp.concatenate([kv[:, 256:384], kv[:, 384:512]], axis=2).reshape(64, 2, 64, 256)

    def scores_of(kb):
        return jnp.einsum("qhgd,khd->hgqk", qn, kb, preferred_element_type=jnp.float32) * 0.125

    def largest(m, kb):
        return jnp.maximum(m, jnp.max(scores_of(kb), axis=-1)), None

    top, _ = lax.scan(largest, jnp.full((2, 4, 256), -1e30, jnp.float32), k)

    def add(carry, block):
        total, summed = carry
        kb, vb = block
        ex = jnp.exp(scores_of(kb) - top[..., None])
        summed += jnp.einsum(
            "hgqk,hdk->hgqd", ex.astype(jnp.bfloat16), vb, preferred_element_type=jnp.float32
        )
        return (total + jnp.sum(ex, axis=-1), summed), None

    zero = (jnp.zeros((2, 4, 256), jnp.float32), jnp.zeros((2, 4, 256, 64), jnp.float32))
    (total, summed), _ = lax.scan(add, zero, (k, v))
    out = jnp.transpose(summed / total[..., None], (2, 0, 1, 3))
    return out.reshape(256, 512).astype(jnp.bfloat16)


SLOTS = 6
PLANE = 16 * SLOTS
OWN = 10


def experts_kernel(
    att_ref, resid_ref, pg_ref, fg_ref, pfg_ref, ids_ref, rw_ref, ow_ref, owp_ref, gate_hbm, up_hbm, down_hbm, o_ref,
    ow, owp, gate, up, down, att_in, hidden, out, arr, x, inner, part, part_out, part_in, total, ret, combined, tiles,
    w_sem, a_sem, d_send, d_recv, f_send, f_recv, p_send, p_recv, r_send, r_recv,
):
    me, core = lax.axis_index("sp"), lax.axis_index("tp")
    other = 1 - core
    f32, bf16 = jnp.float32, jnp.bfloat16

    barrier = pltpu.get_barrier_semaphore()

    def greet(i, carry):
        pl.semaphore_signal(barrier, inc=1, device_id=((me + i) % 64, core), device_id_type=MESH_ID)
        return carry

    lax.fori_loop(1, 64, greet, 0)
    pl.semaphore_signal(barrier, inc=1, device_id=(me, other), device_id_type=MESH_ID)
    loads = [
        pltpu.make_async_copy(src, dst, w_sem.at[i])
        for i, (src, dst) in enumerate(
            ((ow_ref, ow), (owp_ref, owp), (gate_hbm.at[0], gate), (up_hbm.at[0], up), (down_hbm.at[0], down))
        )
    ]
    for load in loads:
        load.start()

    expert = lax.broadcasted_iota(jnp.int32, (64, 128), 0)
    chosen = [(ids_ref[k : k + 1, :] == expert).astype(f32) for k in range(2)]
    above = (
        lax.broadcasted_iota(jnp.int32, (128, 128), 0) < lax.broadcasted_iota(jnp.int32, (128, 128), 1)
    ).astype(f32).astype(bf16)
    earlier = [jnp.dot(c.astype(bf16), above, preferred_element_type=f32) for c in chosen]
    earlier[1] = earlier[1] + jnp.sum(chosen[0], axis=1, keepdims=True)
    slot = [
        ids_ref[k : k + 1, :] * SLOTS
        + jnp.sum(earlier[k] * chosen[k], axis=0, keepdims=True).astype(jnp.int32)
        for k in range(2)
    ]
    line = lax.broadcasted_iota(jnp.int32, (PLANE, 128), 0)
    member = (line * 43) // 256

    def offset_of(j, i):
        dz, dy = (i // 4 + 2) % 4, (i % 4 + 2) % 4
        return dz, dy, (j + 8 - dz - dy) % 4

    def chip_at(j, i, sign):
        dz, dy, dx = offset_of(j, i)
        cz = (me // 16 + 4 + sign * dz) % 4
        cy = ((me // 4) % 4 + 4 + sign * dy) % 4
        cx = (me % 4 + 4 + sign * dx) % 4
        return cz * 16 + cy * 4 + cx

    def place_of(j):
        return chip_at(j, member, 1) * SLOTS + line - member * SLOTS

    pl.semaphore_wait(barrier, 64)

    here = pl.ds(pl.multiple_of(core * 128, 128), 128)
    there = pl.ds(pl.multiple_of(other * 128, 128), 128)
    swap = pltpu.make_async_remote_copy(
        src_ref=att_ref.at[there], dst_ref=att_in, send_sem=a_sem.at[0], recv_sem=a_sem.at[1],
        device_id=(me, other), device_id_type=MESH_ID,
    )
    swap.start()
    loads[0].wait()
    mixed = jnp.dot(att_ref[here, :], ow[...], preferred_element_type=f32)
    loads[1].wait()
    swap.wait()
    mixed = mixed + jnp.dot(att_in[...], owp[...], preferred_element_type=f32)
    state = (resid_ref[...].astype(f32) + rms_scale(mixed, pg_ref[...])).astype(bf16)
    hidden[...] = state
    normed = rms_scale(state.astype(f32), fg_ref[...]).astype(bf16)

    def send(src, dst, number, sems, to):
        rows = pl.ds(number * SLOTS, SLOTS)
        return pltpu.make_async_remote_copy(
            src_ref=src.at[rows], dst_ref=dst.at[rows], send_sem=sems[0].at[number], recv_sem=sems[1].at[number],
            device_id=(to, core), device_id_type=MESH_ID,
        )

    def there_copy(j, i):
        return send(out, arr.at[core], j * 16 + i, (d_send, d_recv), chip_at(j, i, 1))

    def back_copy(j, i):
        return send(total, ret, j * 16 + i, (r_send, r_recv), chip_at(j, i, -1))

    def each(j, act):
        def step(i, carry):
            @pl.when(jnp.logical_or(j > 0, i != OWN))
            def _():
                act(j, i)

            return carry

        lax.fori_loop(0, 16, step, 0)

    own = pl.ds(OWN * SLOTS, SLOTS)

    def dispatch(j, carry):
        place = place_of(j)
        picked = ((slot[0] == place).astype(f32) + (slot[1] == place).astype(f32)).astype(bf16)
        rows = jnp.dot(picked, normed, preferred_element_type=f32)
        tiles[...] = rows.astype(bf16).reshape(PLANE, 16, 128)
        out[pl.ds(j * PLANE, PLANE)] = tiles[...]
        each(j, lambda j, i: there_copy(j, i).start())
        return carry

    lax.fori_loop(0, 4, dispatch, 0)
    arr[core, own] = out[own]
    for load in loads[2:]:
        load.wait()

    def forward(j):
        rows = pl.ds(j * PLANE, PLANE)
        return pltpu.make_async_remote_copy(
            src_ref=arr.at[core, rows], dst_ref=arr.at[core, rows], send_sem=f_send.at[j], recv_sem=f_recv.at[j],
            device_id=(me, other), device_id_type=MESH_ID,
        )

    def partial(j):
        return pltpu.make_async_remote_copy(
            src_ref=part_out.at[j], dst_ref=part_in.at[j], send_sem=p_send.at[j], recv_sem=p_recv.at[j],
            device_id=(me, other), device_id_type=MESH_ID,
        )

    def finish(j):
        partial(j).wait_recv()
        rows = (part[j].astype(f32) + part_in[j].astype(f32)).astype(bf16)
        tiles[...] = rows.reshape(PLANE, 16, 128)
        total[pl.ds(j * PLANE, PLANE)] = tiles[...]

        @pl.when(j == 0)
        def _():
            ret[own] = total[own]

        each(j, lambda j, i: back_copy(j, i).start())

    def chunk(j, carry):
        rows = pl.ds(j * PLANE, PLANE)
        each(j, lambda j, i: there_copy(j, i).wait_recv())
        forward(j).start()
        tiles[...] = arr[core, rows]
        x[0:PLANE, :] = tiles[...].reshape(PLANE, 2048)

        @pl.when(j > 0)
        def _():
            finish(j - 1)

        forward(j).wait_recv()
        tiles[...] = arr[other, rows]
        x[PLANE : 2 * PLANE, :] = tiles[...].reshape(PLANE, 2048)
        for n in range(7):
            at = pl.ds(n * 256, 256)
            g = jnp.dot(x[...], gate[:, at], preferred_element_type=f32)
            u = jnp.dot(x[...], up[:, at], preferred_element_type=f32)
            inner[:, at] = (g / (1.0 + jnp.exp(-g)) * u).astype(bf16)
        for n in range(8):
            at = pl.ds(n * 256, 256)
            y = jnp.dot(inner[...], down[:, at], preferred_element_type=f32).astype(bf16)
            part[j, :, at] = y[0:PLANE]
            part_out[j, :, at] = y[PLANE : 2 * PLANE]

        partial(j).start()
        return carry

    lax.fori_loop(0, 4, chunk, 0)
    finish(jnp.int32(3))

    combined[...] = jnp.zeros_like(combined)

    def collect(j, carry):
        each(j, lambda j, i: back_copy(j, i).wait_recv())
        place = place_of(j)
        weight = jnp.where(slot[0] == place, rw_ref[0:1, :], 0.0) + jnp.where(slot[1] == place, rw_ref[1:2, :], 0.0)
        high = weight.astype(bf16)
        low = (weight - high.astype(f32)).astype(bf16)
        tiles[...] = ret[pl.ds(j * PLANE, PLANE)]
        rows = tiles[...].reshape(PLANE, 2048)
        tn = (((0,), (0,)), ((), ()))
        combined[...] += lax.dot_general(high, rows, tn, preferred_element_type=f32) + lax.dot_general(
            low, rows, tn, preferred_element_type=f32
        )
        return carry

    lax.fori_loop(0, 4, collect, 0)
    o_ref[...] = (hidden[...].astype(f32) + rms_scale(combined[...], pfg_ref[...])).astype(bf16)

    def drain(j, carry):
        each(j, lambda j, i: there_copy(j, i).wait_send())
        each(j, lambda j, i: back_copy(j, i).wait_send())
        forward(j).wait_send()
        partial(j).wait_send()
        return carry

    lax.fori_loop(0, 4, drain, 0)


def experts(attended, resid, post_gain, ffn_gain, post_ffn_gain, route_ids, route_w, out_weight, out_weight_other, gate_w, up_w, down_w):
    vmem, hbm = pl.BlockSpec(memory_space=pltpu.VMEM), pl.BlockSpec(memory_space=pltpu.HBM)
    bf16, f32, dma = jnp.bfloat16, jnp.float32, pltpu.SemaphoreType.DMA
    return pl.pallas_call(
        experts_kernel,
        out_shape=jax.ShapeDtypeStruct((128, 2048), bf16),
        in_specs=[vmem] * 7 + [hbm] * 5,
        out_specs=vmem,
        scratch_shapes=[
            pltpu.VMEM((512, 2048), bf16),
            pltpu.VMEM((512, 2048), bf16),
            pltpu.VMEM((2048, 1792), bf16),
            pltpu.VMEM((2048, 1792), bf16),
            pltpu.VMEM((1792, 2048), bf16),
            pltpu.VMEM((128, 512), bf16),
            pltpu.VMEM((128, 2048), bf16),
            pltpu.VMEM((384, 16, 128), bf16),
            pltpu.VMEM((2, 384, 16, 128), bf16),
            pltpu.VMEM((2 * PLANE, 2048), bf16),
            pltpu.VMEM((2 * PLANE, 1792), bf16),
            pltpu.VMEM((4, PLANE, 2048), bf16),
            pltpu.VMEM((4, PLANE, 2048), bf16),
            pltpu.VMEM((4, PLANE, 2048), bf16),
            pltpu.VMEM((384, 16, 128), bf16),
            pltpu.VMEM((384, 16, 128), bf16),
            pltpu.VMEM((128, 2048), f32),
            pltpu.VMEM((PLANE, 16, 128), bf16),
            dma((5,)), dma((2,)), dma((64,)), dma((64,)), dma((4,)), dma((4,)), dma((4,)), dma((4,)),
            dma((64,)), dma((64,)),
        ],
        compiler_params=pltpu.CompilerParams(
            collective_id=1, has_side_effects=True, vmem_limit_bytes=60 << 20
        ),
        cost_estimate=pl.CostEstimate(flops=20_000_000_000, bytes_accessed=28_000_000, transcendentals=0),
        name="experts",
    )(
        attended, resid, post_gain[None], ffn_gain[None], post_ffn_gain[None], route_ids.T, route_w.T,
        out_weight, out_weight_other, gate_w, up_w, down_w,
    )


def per_device(
    queries,
    keys,
    values,
    q_gain,
    k_gain,
    resid,
    out_weight,
    post_gain,
    ffn_gain,
    post_ffn_gain,
    gate_w,
    up_w,
    down_w,
    route_ids,
    route_w,
):
    attended, den, kv, out_weight_other = attention(queries, keys, values, q_gain, k_gain, out_weight)
    attended = lax.cond(
        den[0, 0] < LIMIT,
        lambda: attended,
        lambda: attention_again(queries, q_gain, kv),
    )
    return experts(
        attended, resid, post_gain, ffn_gain, post_ffn_gain, route_ids, route_w, out_weight, out_weight_other,
        gate_w, up_w, down_w,
    )


def solution(mesh):
    in_specs = (
        P("sp", "tp"),
        P("sp", "tp"),
        P("sp", "tp"),
        P(),
        P(),
        P(("sp", "tp"), None),
        P("tp", None),
        P(),
        P(),
        P(),
        P("sp", None, "tp"),
        P("sp", None, "tp"),
        P("sp", "tp", None),
        P(("sp", "tp"), None),
        P(("sp", "tp"), None),
    )
    out_specs = P(("sp", "tp"), None)
    return jax.shard_map(
        per_device, mesh=mesh, in_specs=in_specs, out_specs=out_specs, check_vma=False
    )
```

```python
import jax
import jax.numpy as jnp
from jax import lax
from jax.experimental import pallas as pl
from jax.experimental.pallas import tpu as pltpu
from jax.sharding import PartitionSpec as P

HEAD_DIM = 64
GRID_W = 64


EPS = 1e-06
THETA = 10000.0


def qk_prepare(raw, gain, positions, head_count):
    count_rows = raw.shape[0]
    values32 = raw.astype(jnp.float32).reshape(count_rows, head_count, HEAD_DIM)
    normed = (
        values32 * lax.rsqrt(jnp.mean(values32 * values32, axis=-1, keepdims=True) + EPS) * gain
    )
    half_dim = HEAD_DIM // 2
    freqs = THETA ** (-jnp.arange(0, half_dim, 2, dtype=jnp.float32) / half_dim)
    grid_row = (positions // GRID_W).astype(jnp.float32)
    grid_col = (positions % GRID_W).astype(jnp.float32)
    angles = jnp.concatenate([grid_row[:, None] * freqs, grid_col[:, None] * freqs], axis=-1)
    cosine = jnp.cos(angles)[:, None, :]
    sine = jnp.sin(angles)[:, None, :]
    paired = normed.reshape(count_rows, head_count, half_dim, 2)
    first = paired[..., 0]
    second = paired[..., 1]
    turned = jnp.stack([first * cosine - second * sine, first * sine + second * cosine], axis=-1)
    return turned.reshape(count_rows, head_count * HEAD_DIM).astype(jnp.bfloat16)


def rms_scale(values32, gain):
    return values32 * lax.rsqrt(jnp.mean(values32 * values32, axis=-1, keepdims=True) + EPS) * gain


MESH_ID = pl.DeviceIdType.MESH
LIMIT = 2.0**100
QSCALE = 1.4426950408889634 / 8.0
ORDER = [0, 12, 48, 4, 16, 3, 1, 60, 28, 8, 52, 15, 32, 19, 2, 51, 5, 7, 20, 17, 13, 49, 56, 11, 24, 18, 35, 21, 6, 29, 36, 50, 55, 44, 23, 9, 33, 14, 61, 63, 25, 53, 59, 39, 45, 40, 10, 62, 34, 22, 27, 47, 41, 58, 57, 30, 38, 54, 43, 37, 31, 26, 46, 42]
PARTS = ((0, 176), (176, 176), (352, 160))


def digits(offset):
    return (offset // 16, offset // 4 % 4, offset % 4)


def onward(offset, part):
    place = digits(offset)
    axes = [(part + i) % 3 for i in range(3)]
    last = max([i for i in range(3) if place[axes[i]]], default=-1)
    out = []
    if last >= 0:
        came = place[axes[last]]
        if came == (1, 3)[(sum(place) - came + part) % 2]:
            out.append((axes[last], came))
    for axis in axes[last + 1 :]:
        out += [(axis, 1), (axis, 3)]
    return out


def relay_plan():
    plan = [[(o, r) for r in range(3) for o in ORDER[1:7]]]
    for g in range(1, 16):
        plan.append([(o, r) for o in ORDER[4 * g + 3 : 4 * g + 7] for r in range(3)])
    return plan


def packed():
    return [sum(ORDER[4 * g + j] * 64**j for j in range(4)) for g in range(16)]


def lookup(words, g):
    w = jnp.int32(words[0])
    for i in range(1, len(words)):
        w = jnp.where(g == i, jnp.int32(words[i]), w)
    return w


def source_of(offset, me):
    cz = (me // 16 + 4 - offset // 16) % 4
    cy = ((me // 4) % 4 + 4 - (offset // 4) % 4) % 4
    cx = (me % 4 + 4 - offset % 4) % 4
    return cz * 16 + cy * 4 + cx


def rows_of(src, start, count):
    return pl.ds(pl.multiple_of(src * 512 + start, 16), count)


def turned_heads(x, gain, cosine, sine):
    out = []
    for h in range(2):
        even, odd = x[64 * h : 64 * h + 32], x[64 * h + 32 : 64 * h + 64]
        squares = jnp.sum(even * even, axis=0, keepdims=True) + jnp.sum(odd * odd, axis=0, keepdims=True)
        scale = lax.rsqrt(squares * (1.0 / 64.0) + EPS)
        even, odd = even * scale * gain[0:32], odd * scale * gain[32:64]
        out.append(jnp.concatenate([even * cosine - odd * sine, even * sine + odd * cosine], axis=0))
    return out


def attention_kernel(
    q_ref, k_ref, v_ref, qg_ref, kg_ref, ow_ref, o_ref, den_ref, kv_out, ow_out,
    qt, top, acc, kv, send_sem, recv_sem, out_sem, swap_sem,
):
    me, core = lax.axis_index("sp"), lax.axis_index("tp")
    coords = (me // 16, (me // 4) % 4, me % 4)
    peers = {
        (axis, step): me + ((coords[axis] + step) % 4 - coords[axis]) * (16, 4, 1)[axis]
        for axis in range(3)
        for step in (1, 3)
    }
    barrier = pltpu.get_barrier_semaphore()
    for to in peers.values():
        pl.semaphore_signal(barrier, inc=1, device_id=(to, core), device_id_type=MESH_ID)
    pl.semaphore_signal(barrier, inc=1, device_id=(me, 1 - core), device_id_type=MESH_ID)

    row = lax.broadcasted_iota(jnp.int32, (128, 128), 0)
    col = lax.broadcasted_iota(jnp.int32, (128, 128), 1)
    within = row % 64
    wanted = (row // 64) * 64 + 2 * (within % 32) + within // 32
    order = (col == wanted).astype(jnp.float32).astype(jnp.bfloat16)
    same = (col == row).astype(jnp.float32).astype(jnp.bfloat16)
    nt = (((1,), (1,)), ((), ()))

    pair = lax.broadcasted_iota(jnp.int32, (32, 256), 0)
    token = lax.broadcasted_iota(jnp.int32, (32, 256), 1)
    freq = jnp.zeros((32, 256), jnp.float32)
    for i in range(16):
        freq = jnp.where(pair % 16 == i, jnp.float32(THETA ** (-i / 16.0)), freq)
    where = jnp.where(pair < 16, me * 4 + token // 64, token % 64)
    angle = where.astype(jnp.float32) * freq
    cosine, sine = jnp.cos(angle), jnp.sin(angle)

    def column(ref):
        return jnp.sum(jnp.where((col == wanted)[0:64, 0:64], ref[...], 0.0), axis=1, keepdims=True)

    kt = turned_heads(
        lax.dot_general(order, k_ref[...], nt, preferred_element_type=jnp.float32), column(kg_ref), cosine, sine
    )
    kv[rows_of(me, 0, 256), :] = jnp.concatenate(kt, axis=0).T.astype(jnp.bfloat16)
    vt = lax.dot_general(same, v_ref[...], nt, preferred_element_type=jnp.float32).astype(jnp.bfloat16)
    kv[rows_of(me, 256, 128), :] = vt[:, 0:128]
    kv[rows_of(me, 384, 128), :] = vt[:, 128:256]

    pl.semaphore_wait(barrier, 7)

    def copy(src, part, to, first):
        rows = rows_of(src, *PARTS[part])
        return pltpu.make_async_remote_copy(
            src_ref=kv.at[rows], dst_ref=kv.at[rows],
            send_sem=send_sem.at[part], recv_sem=recv_sem.at[part if first else 0, src],
            device_id=(to, core), device_id_type=MESH_ID,
        )

    def whole(src):
        rows = rows_of(src, 0, 512)
        return pltpu.make_async_remote_copy(
            src_ref=kv.at[rows], dst_ref=kv.at[rows], send_sem=send_sem.at[0], recv_sem=recv_sem.at[0, src],
            device_id=(me, core), device_id_type=MESH_ID,
        )

    def pass_on(src, offset, part):
        for way in onward(offset, part):
            copy(src, part, peers[way], offset == 0).start()

    def put_out(s):
        rows = rows_of(s, 0, 512)
        return pltpu.make_async_copy(kv.at[rows], kv_out.at[rows], out_sem.at[0])

    for part in range(3):
        pass_on(me, 0, part)
    swap = pltpu.make_async_remote_copy(
        src_ref=ow_ref, dst_ref=ow_out, send_sem=swap_sem.at[0], recv_sem=swap_sem.at[1],
        device_id=(me, 1 - core), device_id_type=MESH_ID,
    )

    qt[...] = jnp.zeros_like(qt)
    q_gain = column(qg_ref)
    for j in range(4):
        heads = turned_heads(
            lax.dot_general(
                order, q_ref[:, 128 * j : 128 * j + 128], nt, preferred_element_type=jnp.float32
            ),
            q_gain, cosine, sine,
        )
        for i in range(2):
            scaled = heads[i].astype(jnp.bfloat16).astype(jnp.float32) * QSCALE
            high = scaled.astype(jnp.bfloat16)
            low = (scaled - high.astype(jnp.float32)).astype(jnp.bfloat16)
            at, to = pl.ds((2 * j + i) * 256, 256), 64 * (j // 2)
            qt[to : to + 64, at] = high
            qt[128 + to : 192 + to, at] = low

    own = kv[rows_of(me, 0, 256), :]
    own = jnp.concatenate([own, own], axis=1)
    for t in range(4):
        at = pl.ds(t * 512, 512)
        s = jnp.dot(own, qt[:, at], preferred_element_type=jnp.float32)
        top[:, at] = jnp.broadcast_to(jnp.max(s, axis=0, keepdims=True), (8, 512))
    acc[...] = jnp.zeros_like(acc)
    ones = jnp.ones((16, 1024), jnp.bfloat16)

    words = packed()
    plan = relay_plan()

    def group(g, carry):
        for i, pieces in enumerate(plan):

            @pl.when(g == i)
            def _():
                for offset, part in pieces:
                    src = source_of(offset, me)
                    if i == 0:
                        copy(src, part, me, True).wait_recv()
                    elif part == 0:
                        whole(src).wait_recv()
                    pass_on(src, offset, part)
                if i == 1:
                    swap.start()

        now = lookup(words, g)
        srcs = [source_of((now // 64**j) % 64, me) for j in range(4)]
        for s in srcs:
            put_out(s).start()
        kk = jnp.concatenate([kv[rows_of(s, 0, 256), :] for s in srcs], axis=0)
        kk = jnp.concatenate([kk, kk], axis=1)
        vt = jnp.concatenate([kv[rows_of(s, a, 128), :] for s in srcs for a in (256, 384)], axis=1)
        va = [jnp.concatenate([vt[64 * h : 64 * h + 64], ones], axis=0) for h in range(2)]
        for t in range(4):
            at = pl.ds(t * 512, 512)
            s = jnp.dot(kk, qt[:, at], preferred_element_type=jnp.float32)
            p = jnp.exp2(s - top[0:1, at]).astype(jnp.bfloat16)
            acc[:, at] += jnp.dot(va[t // 2], p, preferred_element_type=jnp.float32)
        return carry

    lax.fori_loop(0, 16, group, 0)

    for j in range(4):
        parts = []
        for i in range(2):
            at = pl.ds((2 * j + i) * 256, 256)
            parts.append(acc[0:64, at] / acc[64:65, at])
        o_ref[:, 128 * j : 128 * j + 128] = jnp.concatenate(parts, axis=0).T.astype(jnp.bfloat16)
    den_ref[0, 0] = jnp.max(acc[64:65, :])

    for part in range(3):
        sent = kv.at[pl.ds(0, 63 * PARTS[part][1])]
        pltpu.make_async_remote_copy(
            src_ref=sent, dst_ref=sent, send_sem=send_sem.at[part], recv_sem=recv_sem.at[part, 0],
            device_id=(me, core), device_id_type=MESH_ID,
        ).wait_send()
    pltpu.make_async_copy(kv, kv_out, out_sem.at[0]).wait()
    swap.wait()


def attention(queries, keys, values, q_gain, k_gain, out_weight):
    vmem, hbm = pl.BlockSpec(memory_space=pltpu.VMEM), pl.BlockSpec(memory_space=pltpu.HBM)
    return pl.pallas_call(
        attention_kernel,
        out_shape=(
            jax.ShapeDtypeStruct((256, 512), jnp.bfloat16),
            jax.ShapeDtypeStruct((1, 1), jnp.float32),
            jax.ShapeDtypeStruct((64 * 512, 128), jnp.bfloat16),
            jax.ShapeDtypeStruct((512, 2048), jnp.bfloat16),
        ),
        in_specs=[vmem] * 5 + [hbm],
        out_specs=(vmem, pl.BlockSpec(memory_space=pltpu.SMEM), hbm, hbm),
        scratch_shapes=[
            pltpu.VMEM((256, 2048), jnp.bfloat16),
            pltpu.VMEM((8, 2048), jnp.float32),
            pltpu.VMEM((80, 2048), jnp.float32),
            pltpu.VMEM((64 * 512, 128), jnp.bfloat16),
            pltpu.SemaphoreType.DMA((3,)),
            pltpu.SemaphoreType.DMA((3, 64)),
            pltpu.SemaphoreType.DMA((1,)),
            pltpu.SemaphoreType.DMA((2,)),
        ],
        compiler_params=pltpu.CompilerParams(
            collective_id=0, has_side_effects=True, vmem_limit_bytes=56 << 20
        ),
        cost_estimate=pl.CostEstimate(flops=17_000_000_000, bytes_accessed=9_000_000, transcendentals=0),
        name="attention",
    )(queries, keys, values, q_gain[None], k_gain[None], out_weight)


def attention_again(queries, q_gain, kv):
    me = lax.axis_index("sp")
    positions = me * 256 + jnp.arange(256, dtype=jnp.int32)
    qn = qk_prepare(queries, q_gain, positions, 8).reshape(256, 2, 4, 32, 2)
    qn = jnp.swapaxes(qn, -1, -2).reshape(256, 2, 4, 64)
    kv = kv.reshape(64, 512, 128)
    k = kv[:, 0:256].reshape(64, 256, 2, 64)
    v = jnp.concatenate([kv[:, 256:384], kv[:, 384:512]], axis=2).reshape(64, 2, 64, 256)

    def scores_of(kb):
        return jnp.einsum("qhgd,khd->hgqk", qn, kb, preferred_element_type=jnp.float32) * 0.125

    def largest(m, kb):
        return jnp.maximum(m, jnp.max(scores_of(kb), axis=-1)), None

    top, _ = lax.scan(largest, jnp.full((2, 4, 256), -1e30, jnp.float32), k)

    def add(carry, block):
        total, summed = carry
        kb, vb = block
        ex = jnp.exp(scores_of(kb) - top[..., None])
        summed += jnp.einsum(
            "hgqk,hdk->hgqd", ex.astype(jnp.bfloat16), vb, preferred_element_type=jnp.float32
        )
        return (total + jnp.sum(ex, axis=-1), summed), None

    zero = (jnp.zeros((2, 4, 256), jnp.float32), jnp.zeros((2, 4, 256, 64), jnp.float32))
    (total, summed), _ = lax.scan(add, zero, (k, v))
    out = jnp.transpose(summed / total[..., None], (2, 0, 1, 3))
    return out.reshape(256, 512).astype(jnp.bfloat16)


SLOTS = 6
PLANE = 16 * SLOTS
OWN = 10


def experts_kernel(
    att_ref, resid_ref, pg_ref, fg_ref, pfg_ref, ids_ref, rw_ref, ow_ref, owp_ref, gate_hbm, up_hbm, down_hbm, o_ref,
    ow, owp, gate, up, down, att_in, hidden, out, arr, x, inner, part, part_out, part_in, total, ret, combined, tiles,
    w_sem, a_sem, d_send, d_recv, f_send, f_recv, p_send, p_recv, r_send, r_recv,
):
    me, core = lax.axis_index("sp"), lax.axis_index("tp")
    other = 1 - core
    f32, bf16 = jnp.float32, jnp.bfloat16

    barrier = pltpu.get_barrier_semaphore()

    def greet(i, carry):
        pl.semaphore_signal(barrier, inc=1, device_id=((me + i) % 64, core), device_id_type=MESH_ID)
        return carry

    lax.fori_loop(1, 64, greet, 0)
    pl.semaphore_signal(barrier, inc=1, device_id=(me, other), device_id_type=MESH_ID)
    loads = [
        pltpu.make_async_copy(src, dst, w_sem.at[i])
        for i, (src, dst) in enumerate(
            ((ow_ref, ow), (owp_ref, owp), (gate_hbm.at[0], gate), (up_hbm.at[0], up), (down_hbm.at[0], down))
        )
    ]
    for load in loads:
        load.start()

    expert = lax.broadcasted_iota(jnp.int32, (64, 128), 0)
    chosen = [(ids_ref[k : k + 1, :] == expert).astype(f32) for k in range(2)]
    above = (
        lax.broadcasted_iota(jnp.int32, (128, 128), 0) < lax.broadcasted_iota(jnp.int32, (128, 128), 1)
    ).astype(f32).astype(bf16)
    earlier = [jnp.dot(c.astype(bf16), above, preferred_element_type=f32) for c in chosen]
    earlier[1] = earlier[1] + jnp.sum(chosen[0], axis=1, keepdims=True)
    slot = [
        ids_ref[k : k + 1, :] * SLOTS
        + jnp.sum(earlier[k] * chosen[k], axis=0, keepdims=True).astype(jnp.int32)
        for k in range(2)
    ]
    line = lax.broadcasted_iota(jnp.int32, (PLANE, 128), 0)
    member = (line * 43) // 256

    def offset_of(j, i):
        dz, dy = (i // 4 + 2) % 4, (i % 4 + 2) % 4
        return dz, dy, (j + 8 - dz - dy) % 4

    def chip_at(j, i, sign):
        dz, dy, dx = offset_of(j, i)
        cz = (me // 16 + 4 + sign * dz) % 4
        cy = ((me // 4) % 4 + 4 + sign * dy) % 4
        cx = (me % 4 + 4 + sign * dx) % 4
        return cz * 16 + cy * 4 + cx

    def place_of(j):
        return chip_at(j, member, 1) * SLOTS + line - member * SLOTS

    here = pl.ds(pl.multiple_of(core * 128, 128), 128)
    there = pl.ds(pl.multiple_of(other * 128, 128), 128)
    loads[0].wait()
    mixed = jnp.dot(att_ref[here, :], ow[...], preferred_element_type=f32)

    pl.semaphore_wait(barrier, 64)
    swap = pltpu.make_async_remote_copy(
        src_ref=att_ref.at[there], dst_ref=att_in, send_sem=a_sem.at[0], recv_sem=a_sem.at[1],
        device_id=(me, other), device_id_type=MESH_ID,
    )
    swap.start()
    loads[1].wait()
    swap.wait()
    mixed = mixed + jnp.dot(att_in[...], owp[...], preferred_element_type=f32)
    state = (resid_ref[...].astype(f32) + rms_scale(mixed, pg_ref[...])).astype(bf16)
    hidden[...] = state
    normed = rms_scale(state.astype(f32), fg_ref[...]).astype(bf16)

    def send(src, dst, j, rows, sems, to):
        return pltpu.make_async_remote_copy(
            src_ref=src.at[rows], dst_ref=dst.at[rows], send_sem=sems[0].at[j], recv_sem=sems[1].at[j],
            device_id=(to, core), device_id_type=MESH_ID,
        )

    def member_rows(j, i):
        return pl.ds((j * 16 + i) * SLOTS, SLOTS)

    def there_copy(j, i):
        return send(out, arr.at[core], j, member_rows(j, i), (d_send, d_recv), chip_at(j, i, 1))

    def back_copy(j, i):
        return send(total, ret, j, member_rows(j, i), (r_send, r_recv), chip_at(j, i, -1))

    def each(j, act):
        for i in range(16):
            if i == OWN:
                pl.when(j > 0)(lambda: act(j, OWN))
            else:
                act(j, i)

    def all_there(j, count):
        return send(out, arr.at[core], j, pl.ds(0, count * SLOTS), (d_send, d_recv), me)

    def all_back(j, count):
        return send(total, ret, j, pl.ds(0, count * SLOTS), (r_send, r_recv), me)

    def once(j, act):
        pl.when(j == 0)(lambda: act(15))
        pl.when(j > 0)(lambda: act(16))

    own = pl.ds(OWN * SLOTS, SLOTS)

    def dispatch(j, carry):
        place = place_of(j)
        picked = ((slot[0] == place).astype(f32) + (slot[1] == place).astype(f32)).astype(bf16)
        rows = jnp.dot(picked, normed, preferred_element_type=f32)
        tiles[...] = rows.astype(bf16).reshape(PLANE, 16, 128)
        out[pl.ds(j * PLANE, PLANE)] = tiles[...]
        each(j, lambda j, i: there_copy(j, i).start())
        return carry

    lax.fori_loop(0, 4, dispatch, 0)
    arr[core, own] = out[own]
    for load in loads[2:]:
        load.wait()

    def forward(j):
        rows = pl.ds(j * PLANE, PLANE)
        return pltpu.make_async_remote_copy(
            src_ref=arr.at[core, rows], dst_ref=arr.at[core, rows], send_sem=f_send.at[j], recv_sem=f_recv.at[j],
            device_id=(me, other), device_id_type=MESH_ID,
        )

    def partial(j):
        return pltpu.make_async_remote_copy(
            src_ref=part_out.at[j], dst_ref=part_in.at[j], send_sem=p_send.at[j], recv_sem=p_recv.at[j],
            device_id=(me, other), device_id_type=MESH_ID,
        )

    def finish(j):
        partial(j).wait_recv()
        rows = (part[j].astype(f32) + part_in[j].astype(f32)).astype(bf16)
        tiles[...] = rows.reshape(PLANE, 16, 128)
        total[pl.ds(j * PLANE, PLANE)] = tiles[...]

        @pl.when(j == 0)
        def _():
            ret[own] = total[own]

        each(j, lambda j, i: back_copy(j, i).start())

    def receive(j):
        once(j, lambda count: all_there(j, count).wait_recv())
        forward(j).start()

    def unpack_own(j):
        tiles[...] = arr[core, pl.ds(j * PLANE, PLANE)]
        x[0:PLANE, :] = tiles[...].reshape(PLANE, 2048)

    def unpack_other(j):
        rows = pl.ds(j * PLANE, PLANE)
        forward(j).wait_recv()
        tiles[...] = arr[other, rows]
        x[PLANE : 2 * PLANE, :] = tiles[...].reshape(PLANE, 2048)

    receive(jnp.int32(0))
    unpack_own(jnp.int32(0))
    unpack_other(jnp.int32(0))

    def chunk(j, carry):
        for n in range(7):
            at = pl.ds(n * 256, 256)
            g = jnp.dot(x[...], gate[:, at], preferred_element_type=f32)
            u = jnp.dot(x[...], up[:, at], preferred_element_type=f32)
            inner[:, at] = (g / (1.0 + jnp.exp(-g)) * u).astype(bf16)

        @pl.when(j > 0)
        def _():
            finish(j - 1)

        @pl.when(j < 3)
        def _():
            receive(j + 1)

        unpack_own(jnp.minimum(j + 1, 3))
        for n in range(8):
            at = pl.ds(n * 256, 256)
            y = jnp.dot(inner[...], down[:, at], preferred_element_type=f32).astype(bf16)
            part[j, :, at] = y[0:PLANE]
            part_out[j, :, at] = y[PLANE : 2 * PLANE]

        partial(j).start()

        @pl.when(j < 3)
        def _():
            unpack_other(j + 1)

        return carry

    lax.fori_loop(0, 4, chunk, 0)
    finish(jnp.int32(3))

    combined[...] = jnp.zeros_like(combined)

    def collect(j, carry):
        once(j, lambda count: all_back(j, count).wait_recv())
        place = place_of(j)
        weight = jnp.where(slot[0] == place, rw_ref[0:1, :], 0.0) + jnp.where(slot[1] == place, rw_ref[1:2, :], 0.0)
        high = weight.astype(bf16)
        low = (weight - high.astype(f32)).astype(bf16)
        tiles[...] = ret[pl.ds(j * PLANE, PLANE)]
        rows = tiles[...].reshape(PLANE, 2048)
        tn = (((0,), (0,)), ((), ()))
        combined[...] += lax.dot_general(high, rows, tn, preferred_element_type=f32) + lax.dot_general(
            low, rows, tn, preferred_element_type=f32
        )
        return carry

    lax.fori_loop(0, 4, collect, 0)
    o_ref[...] = (hidden[...].astype(f32) + rms_scale(combined[...], pfg_ref[...])).astype(bf16)

    def drain(j, carry):
        once(j, lambda count: all_there(j, count).wait_send())
        once(j, lambda count: all_back(j, count).wait_send())
        forward(j).wait_send()
        partial(j).wait_send()
        return carry

    lax.fori_loop(0, 4, drain, 0)


def experts(attended, resid, post_gain, ffn_gain, post_ffn_gain, route_ids, route_w, out_weight, out_weight_other, gate_w, up_w, down_w):
    vmem, hbm = pl.BlockSpec(memory_space=pltpu.VMEM), pl.BlockSpec(memory_space=pltpu.HBM)
    bf16, f32, dma = jnp.bfloat16, jnp.float32, pltpu.SemaphoreType.DMA
    return pl.pallas_call(
        experts_kernel,
        out_shape=jax.ShapeDtypeStruct((128, 2048), bf16),
        in_specs=[vmem] * 7 + [hbm] * 5,
        out_specs=vmem,
        scratch_shapes=[
            pltpu.VMEM((512, 2048), bf16),
            pltpu.VMEM((512, 2048), bf16),
            pltpu.VMEM((2048, 1792), bf16),
            pltpu.VMEM((2048, 1792), bf16),
            pltpu.VMEM((1792, 2048), bf16),
            pltpu.VMEM((128, 512), bf16),
            pltpu.VMEM((128, 2048), bf16),
            pltpu.VMEM((384, 16, 128), bf16),
            pltpu.VMEM((2, 384, 16, 128), bf16),
            pltpu.VMEM((2 * PLANE, 2048), bf16),
            pltpu.VMEM((2 * PLANE, 1792), bf16),
            pltpu.VMEM((4, PLANE, 2048), bf16),
            pltpu.VMEM((4, PLANE, 2048), bf16),
            pltpu.VMEM((4, PLANE, 2048), bf16),
            pltpu.VMEM((384, 16, 128), bf16),
            pltpu.VMEM((384, 16, 128), bf16),
            pltpu.VMEM((128, 2048), f32),
            pltpu.VMEM((PLANE, 16, 128), bf16),
            dma((5,)), dma((2,)), dma((4,)), dma((4,)), dma((4,)), dma((4,)), dma((4,)), dma((4,)),
            dma((4,)), dma((4,)),
        ],
        compiler_params=pltpu.CompilerParams(
            collective_id=1, has_side_effects=True, vmem_limit_bytes=62 << 20
        ),
        cost_estimate=pl.CostEstimate(flops=20_000_000_000, bytes_accessed=28_000_000, transcendentals=0),
        name="experts",
    )(
        attended, resid, post_gain[None], ffn_gain[None], post_ffn_gain[None], route_ids.T, route_w.T,
        out_weight, out_weight_other, gate_w, up_w, down_w,
    )


def per_device(
    queries,
    keys,
    values,
    q_gain,
    k_gain,
    resid,
    out_weight,
    post_gain,
    ffn_gain,
    post_ffn_gain,
    gate_w,
    up_w,
    down_w,
    route_ids,
    route_w,
):
    attended, den, kv, out_weight_other = attention(queries, keys, values, q_gain, k_gain, out_weight)
    attended = lax.cond(
        den[0, 0] < LIMIT,
        lambda: attended,
        lambda: attention_again(queries, q_gain, kv),
    )
    return experts(
        attended, resid, post_gain, ffn_gain, post_ffn_gain, route_ids, route_w, out_weight, out_weight_other,
        gate_w, up_w, down_w,
    )


def solution(mesh):
    in_specs = (
        P("sp", "tp"),
        P("sp", "tp"),
        P("sp", "tp"),
        P(),
        P(),
        P(("sp", "tp"), None),
        P("tp", None),
        P(),
        P(),
        P(),
        P("sp", None, "tp"),
        P("sp", None, "tp"),
        P("sp", "tp", None),
        P(("sp", "tp"), None),
        P(("sp", "tp"), None),
    )
    out_specs = P(("sp", "tp"), None)
    return jax.shard_map(
        per_device, mesh=mesh, in_specs=in_specs, out_specs=out_specs, check_vma=False
    )
```

```python
import jax
import jax.numpy as jnp
from jax import lax
from jax.experimental import pallas as pl
from jax.experimental.pallas import tpu as pltpu
from jax.sharding import PartitionSpec as P

HEAD_DIM = 64
GRID_W = 64


EPS = 1e-06
THETA = 10000.0


def qk_prepare(raw, gain, positions, head_count):
    count_rows = raw.shape[0]
    values32 = raw.astype(jnp.float32).reshape(count_rows, head_count, HEAD_DIM)
    normed = (
        values32 * lax.rsqrt(jnp.mean(values32 * values32, axis=-1, keepdims=True) + EPS) * gain
    )
    half_dim = HEAD_DIM // 2
    freqs = THETA ** (-jnp.arange(0, half_dim, 2, dtype=jnp.float32) / half_dim)
    grid_row = (positions // GRID_W).astype(jnp.float32)
    grid_col = (positions % GRID_W).astype(jnp.float32)
    angles = jnp.concatenate([grid_row[:, None] * freqs, grid_col[:, None] * freqs], axis=-1)
    cosine = jnp.cos(angles)[:, None, :]
    sine = jnp.sin(angles)[:, None, :]
    paired = normed.reshape(count_rows, head_count, half_dim, 2)
    first = paired[..., 0]
    second = paired[..., 1]
    turned = jnp.stack([first * cosine - second * sine, first * sine + second * cosine], axis=-1)
    return turned.reshape(count_rows, head_count * HEAD_DIM).astype(jnp.bfloat16)


def rms_scale(values32, gain):
    return values32 * lax.rsqrt(jnp.mean(values32 * values32, axis=-1, keepdims=True) + EPS) * gain


MESH_ID = pl.DeviceIdType.MESH
LIMIT = 2.0**100
QSCALE = 1.4426950408889634 / 8.0
ORDER = [0, 12, 48, 4, 16, 3, 1, 60, 28, 8, 52, 15, 32, 19, 2, 51, 5, 7, 20, 17, 13, 49, 56, 11, 24, 18, 35, 21, 6, 29, 36, 50, 55, 44, 23, 9, 33, 14, 61, 63, 25, 53, 59, 39, 45, 40, 10, 62, 34, 22, 27, 47, 41, 58, 57, 30, 38, 54, 43, 37, 31, 26, 46, 42]
PARTS = ((0, 176), (176, 176), (352, 160))


def digits(offset):
    return (offset // 16, offset // 4 % 4, offset % 4)


def onward(offset, part):
    place = digits(offset)
    axes = [(part + i) % 3 for i in range(3)]
    last = max([i for i in range(3) if place[axes[i]]], default=-1)
    out = []
    if last >= 0:
        came = place[axes[last]]
        if came == (1, 3)[(sum(place) - came + part) % 2]:
            out.append((axes[last], came))
    for axis in axes[last + 1 :]:
        out += [(axis, 1), (axis, 3)]
    return out


def relay_plan():
    plan = [[(o, r) for r in range(3) for o in ORDER[1:7]]]
    for g in range(1, 16):
        plan.append([(o, r) for o in ORDER[4 * g + 3 : 4 * g + 7] for r in range(3)])
    return plan


def packed():
    return [sum(ORDER[4 * g + j] * 64**j for j in range(4)) for g in range(16)]


def lookup(words, g):
    w = jnp.int32(words[0])
    for i in range(1, len(words)):
        w = jnp.where(g == i, jnp.int32(words[i]), w)
    return w


def source_of(offset, me):
    cz = (me // 16 + 4 - offset // 16) % 4
    cy = ((me // 4) % 4 + 4 - (offset // 4) % 4) % 4
    cx = (me % 4 + 4 - offset % 4) % 4
    return cz * 16 + cy * 4 + cx


def rows_of(src, start, count):
    return pl.ds(pl.multiple_of(src * 512 + start, 16), count)


def turned_heads(x, gain, cosine, sine):
    out = []
    for h in range(2):
        even, odd = x[64 * h : 64 * h + 32], x[64 * h + 32 : 64 * h + 64]
        squares = jnp.sum(even * even, axis=0, keepdims=True) + jnp.sum(odd * odd, axis=0, keepdims=True)
        scale = lax.rsqrt(squares * (1.0 / 64.0) + EPS)
        even, odd = even * scale * gain[0:32], odd * scale * gain[32:64]
        out.append(jnp.concatenate([even * cosine - odd * sine, even * sine + odd * cosine], axis=0))
    return out


def attention_kernel(
    q_ref, k_ref, v_ref, qg_ref, kg_ref, ow_ref, o_ref, den_ref, kv_out, ow_out,
    qt, top, acc, kv, send_sem, recv_sem, out_sem, swap_sem,
):
    me, core = lax.axis_index("sp"), lax.axis_index("tp")
    coords = (me // 16, (me // 4) % 4, me % 4)
    peers = {
        (axis, step): me + ((coords[axis] + step) % 4 - coords[axis]) * (16, 4, 1)[axis]
        for axis in range(3)
        for step in (1, 3)
    }
    barrier = pltpu.get_barrier_semaphore()
    for to in peers.values():
        pl.semaphore_signal(barrier, inc=1, device_id=(to, core), device_id_type=MESH_ID)
    pl.semaphore_signal(barrier, inc=1, device_id=(me, 1 - core), device_id_type=MESH_ID)

    row = lax.broadcasted_iota(jnp.int32, (128, 128), 0)
    col = lax.broadcasted_iota(jnp.int32, (128, 128), 1)
    within = row % 64
    wanted = (row // 64) * 64 + 2 * (within % 32) + within // 32
    order = (col == wanted).astype(jnp.float32).astype(jnp.bfloat16)
    same = (col == row).astype(jnp.float32).astype(jnp.bfloat16)
    nt = (((1,), (1,)), ((), ()))

    pair = lax.broadcasted_iota(jnp.int32, (32, 256), 0)
    token = lax.broadcasted_iota(jnp.int32, (32, 256), 1)
    freq = jnp.zeros((32, 256), jnp.float32)
    for i in range(16):
        freq = jnp.where(pair % 16 == i, jnp.float32(THETA ** (-i / 16.0)), freq)
    where = jnp.where(pair < 16, me * 4 + token // 64, token % 64)
    angle = where.astype(jnp.float32) * freq
    cosine, sine = jnp.cos(angle), jnp.sin(angle)

    def column(ref):
        return jnp.sum(jnp.where((col == wanted)[0:64, 0:64], ref[...], 0.0), axis=1, keepdims=True)

    kt = turned_heads(
        lax.dot_general(order, k_ref[...], nt, preferred_element_type=jnp.float32), column(kg_ref), cosine, sine
    )
    kv[rows_of(me, 0, 256), :] = jnp.concatenate(kt, axis=0).T.astype(jnp.bfloat16)
    vt = lax.dot_general(same, v_ref[...], nt, preferred_element_type=jnp.float32).astype(jnp.bfloat16)
    kv[rows_of(me, 256, 128), :] = vt[:, 0:128]
    kv[rows_of(me, 384, 128), :] = vt[:, 128:256]

    pl.semaphore_wait(barrier, 7)

    def copy(src, part, to, first):
        rows = rows_of(src, *PARTS[part])
        return pltpu.make_async_remote_copy(
            src_ref=kv.at[rows], dst_ref=kv.at[rows],
            send_sem=send_sem.at[part], recv_sem=recv_sem.at[part if first else 0, src],
            device_id=(to, core), device_id_type=MESH_ID,
        )

    def whole(src):
        rows = rows_of(src, 0, 512)
        return pltpu.make_async_remote_copy(
            src_ref=kv.at[rows], dst_ref=kv.at[rows], send_sem=send_sem.at[0], recv_sem=recv_sem.at[0, src],
            device_id=(me, core), device_id_type=MESH_ID,
        )

    def pass_on(src, offset, part):
        for way in onward(offset, part):
            copy(src, part, peers[way], offset == 0).start()

    def put_out(s):
        rows = rows_of(s, 0, 512)
        return pltpu.make_async_copy(kv.at[rows], kv_out.at[rows], out_sem.at[0])

    for part in range(3):
        pass_on(me, 0, part)
    swap = pltpu.make_async_remote_copy(
        src_ref=ow_ref, dst_ref=ow_out, send_sem=swap_sem.at[0], recv_sem=swap_sem.at[1],
        device_id=(me, 1 - core), device_id_type=MESH_ID,
    )

    qt[...] = jnp.zeros_like(qt)
    q_gain = column(qg_ref)
    for j in range(4):
        heads = turned_heads(
            lax.dot_general(
                order, q_ref[:, 128 * j : 128 * j + 128], nt, preferred_element_type=jnp.float32
            ),
            q_gain, cosine, sine,
        )
        for i in range(2):
            scaled = heads[i].astype(jnp.bfloat16).astype(jnp.float32) * QSCALE
            high = scaled.astype(jnp.bfloat16)
            low = (scaled - high.astype(jnp.float32)).astype(jnp.bfloat16)
            at, to = pl.ds((2 * j + i) * 256, 256), 64 * (j // 2)
            qt[to : to + 64, at] = high
            qt[128 + to : 192 + to, at] = low

    own = kv[rows_of(me, 0, 256), :]
    own = jnp.concatenate([own, own], axis=1)
    for t in range(4):
        at = pl.ds(t * 512, 512)
        s = jnp.dot(own, qt[:, at], preferred_element_type=jnp.float32)
        top[:, at] = jnp.broadcast_to(jnp.max(s, axis=0, keepdims=True), (8, 512))
    acc[...] = jnp.zeros_like(acc)
    ones = jnp.ones((16, 1024), jnp.bfloat16)

    words = packed()
    plan = relay_plan()

    def group(g, carry):
        for i, pieces in enumerate(plan):

            @pl.when(g == i)
            def _():
                for offset, part in pieces:
                    src = source_of(offset, me)
                    if i == 0:
                        copy(src, part, me, True).wait_recv()
                    elif part == 0:
                        whole(src).wait_recv()
                    pass_on(src, offset, part)
                if i == 1:
                    swap.start()

        now = lookup(words, g)
        srcs = [source_of((now // 64**j) % 64, me) for j in range(4)]
        for s in srcs:
            put_out(s).start()
        kk = jnp.concatenate([kv[rows_of(s, 0, 256), :] for s in srcs], axis=0)
        kk = jnp.concatenate([kk, kk], axis=1)
        vt = jnp.concatenate([kv[rows_of(s, a, 128), :] for s in srcs for a in (256, 384)], axis=1)
        va = [jnp.concatenate([vt[64 * h : 64 * h + 64], ones], axis=0) for h in range(2)]
        for t in range(2):
            at = pl.ds(t * 1024, 1024)
            s = jnp.dot(kk, qt[:, at], preferred_element_type=jnp.float32)
            p = jnp.exp2(s - top[0:1, at]).astype(jnp.bfloat16)
            acc[:, at] += jnp.dot(va[t], p, preferred_element_type=jnp.float32)
        return carry

    lax.fori_loop(0, 16, group, 0)

    for j in range(4):
        parts = []
        for i in range(2):
            at = pl.ds((2 * j + i) * 256, 256)
            parts.append(acc[0:64, at] / acc[64:65, at])
        o_ref[:, 128 * j : 128 * j + 128] = jnp.concatenate(parts, axis=0).T.astype(jnp.bfloat16)
    den_ref[0, 0] = jnp.max(acc[64:65, :])

    for part in range(3):
        sent = kv.at[pl.ds(0, 63 * PARTS[part][1])]
        pltpu.make_async_remote_copy(
            src_ref=sent, dst_ref=sent, send_sem=send_sem.at[part], recv_sem=recv_sem.at[part, 0],
            device_id=(me, core), device_id_type=MESH_ID,
        ).wait_send()
    pltpu.make_async_copy(kv, kv_out, out_sem.at[0]).wait()
    swap.wait()


def attention(queries, keys, values, q_gain, k_gain, out_weight):
    vmem, hbm = pl.BlockSpec(memory_space=pltpu.VMEM), pl.BlockSpec(memory_space=pltpu.HBM)
    return pl.pallas_call(
        attention_kernel,
        out_shape=(
            jax.ShapeDtypeStruct((256, 512), jnp.bfloat16),
            jax.ShapeDtypeStruct((1, 1), jnp.float32),
            jax.ShapeDtypeStruct((64 * 512, 128), jnp.bfloat16),
            jax.ShapeDtypeStruct((512, 2048), jnp.bfloat16),
        ),
        in_specs=[vmem] * 5 + [hbm],
        out_specs=(vmem, pl.BlockSpec(memory_space=pltpu.SMEM), hbm, hbm),
        scratch_shapes=[
            pltpu.VMEM((256, 2048), jnp.bfloat16),
            pltpu.VMEM((8, 2048), jnp.float32),
            pltpu.VMEM((80, 2048), jnp.float32),
            pltpu.VMEM((64 * 512, 128), jnp.bfloat16),
            pltpu.SemaphoreType.DMA((3,)),
            pltpu.SemaphoreType.DMA((3, 64)),
            pltpu.SemaphoreType.DMA((1,)),
            pltpu.SemaphoreType.DMA((2,)),
        ],
        compiler_params=pltpu.CompilerParams(
            collective_id=0, has_side_effects=True, vmem_limit_bytes=56 << 20
        ),
        cost_estimate=pl.CostEstimate(flops=17_000_000_000, bytes_accessed=9_000_000, transcendentals=0),
        name="attention",
    )(queries, keys, values, q_gain[None], k_gain[None], out_weight)


def attention_again(queries, q_gain, kv):
    me = lax.axis_index("sp")
    positions = me * 256 + jnp.arange(256, dtype=jnp.int32)
    qn = qk_prepare(queries, q_gain, positions, 8).reshape(256, 2, 4, 32, 2)
    qn = jnp.swapaxes(qn, -1, -2).reshape(256, 2, 4, 64)
    kv = kv.reshape(64, 512, 128)
    k = kv[:, 0:256].reshape(64, 256, 2, 64)
    v = jnp.concatenate([kv[:, 256:384], kv[:, 384:512]], axis=2).reshape(64, 2, 64, 256)

    def scores_of(kb):
        return jnp.einsum("qhgd,khd->hgqk", qn, kb, preferred_element_type=jnp.float32) * 0.125

    def largest(m, kb):
        return jnp.maximum(m, jnp.max(scores_of(kb), axis=-1)), None

    top, _ = lax.scan(largest, jnp.full((2, 4, 256), -1e30, jnp.float32), k)

    def add(carry, block):
        total, summed = carry
        kb, vb = block
        ex = jnp.exp(scores_of(kb) - top[..., None])
        summed += jnp.einsum(
            "hgqk,hdk->hgqd", ex.astype(jnp.bfloat16), vb, preferred_element_type=jnp.float32
        )
        return (total + jnp.sum(ex, axis=-1), summed), None

    zero = (jnp.zeros((2, 4, 256), jnp.float32), jnp.zeros((2, 4, 256, 64), jnp.float32))
    (total, summed), _ = lax.scan(add, zero, (k, v))
    out = jnp.transpose(summed / total[..., None], (2, 0, 1, 3))
    return out.reshape(256, 512).astype(jnp.bfloat16)


SLOTS = 6
PLANE = 16 * SLOTS
OWN = 10


def experts_kernel(
    att_ref, resid_ref, pg_ref, fg_ref, pfg_ref, ids_ref, rw_ref, ow_ref, owp_ref, gate_hbm, up_hbm, down_hbm, o_ref,
    ow, owp, gate, up, down, att_in, hidden, out, arr, x, inner, part, part_out, part_in, total, ret, combined, tiles,
    w_sem, a_sem, d_send, d_recv, f_send, f_recv, p_send, p_recv, r_send, r_recv,
):
    me, core = lax.axis_index("sp"), lax.axis_index("tp")
    other = 1 - core
    f32, bf16 = jnp.float32, jnp.bfloat16

    barrier = pltpu.get_barrier_semaphore()

    def greet(i, carry):
        pl.semaphore_signal(barrier, inc=1, device_id=((me + i) % 64, core), device_id_type=MESH_ID)
        return carry

    lax.fori_loop(1, 64, greet, 0)
    pl.semaphore_signal(barrier, inc=1, device_id=(me, other), device_id_type=MESH_ID)
    loads = [
        pltpu.make_async_copy(src, dst, w_sem.at[i])
        for i, (src, dst) in enumerate(
            ((ow_ref, ow), (owp_ref, owp), (gate_hbm.at[0], gate), (up_hbm.at[0], up), (down_hbm.at[0], down))
        )
    ]
    for load in loads:
        load.start()

    expert = lax.broadcasted_iota(jnp.int32, (64, 128), 0)
    chosen = [(ids_ref[k : k + 1, :] == expert).astype(f32) for k in range(2)]
    above = (
        lax.broadcasted_iota(jnp.int32, (128, 128), 0) < lax.broadcasted_iota(jnp.int32, (128, 128), 1)
    ).astype(f32).astype(bf16)
    earlier = [jnp.dot(c.astype(bf16), above, preferred_element_type=f32) for c in chosen]
    earlier[1] = earlier[1] + jnp.sum(chosen[0], axis=1, keepdims=True)
    slot = [
        ids_ref[k : k + 1, :] * SLOTS
        + jnp.sum(earlier[k] * chosen[k], axis=0, keepdims=True).astype(jnp.int32)
        for k in range(2)
    ]
    line = lax.broadcasted_iota(jnp.int32, (PLANE, 128), 0)
    member = (line * 43) // 256

    def offset_of(j, i):
        dz, dy = (i // 4 + 2) % 4, (i % 4 + 2) % 4
        return dz, dy, (j + 8 - dz - dy) % 4

    def chip_at(j, i, sign):
        dz, dy, dx = offset_of(j, i)
        cz = (me // 16 + 4 + sign * dz) % 4
        cy = ((me // 4) % 4 + 4 + sign * dy) % 4
        cx = (me % 4 + 4 + sign * dx) % 4
        return cz * 16 + cy * 4 + cx

    def place_of(j):
        return chip_at(j, member, 1) * SLOTS + line - member * SLOTS

    here = pl.ds(pl.multiple_of(core * 128, 128), 128)
    there = pl.ds(pl.multiple_of(other * 128, 128), 128)
    loads[0].wait()
    mixed = jnp.dot(att_ref[here, :], ow[...], preferred_element_type=f32)

    pl.semaphore_wait(barrier, 64)
    swap = pltpu.make_async_remote_copy(
        src_ref=att_ref.at[there], dst_ref=att_in, send_sem=a_sem.at[0], recv_sem=a_sem.at[1],
        device_id=(me, other), device_id_type=MESH_ID,
    )
    swap.start()
    loads[1].wait()
    swap.wait()
    mixed = mixed + jnp.dot(att_in[...], owp[...], preferred_element_type=f32)
    state = (resid_ref[...].astype(f32) + rms_scale(mixed, pg_ref[...])).astype(bf16)
    hidden[...] = state
    normed = rms_scale(state.astype(f32), fg_ref[...]).astype(bf16)

    def send(src, dst, j, rows, sems, to):
        return pltpu.make_async_remote_copy(
            src_ref=src.at[rows], dst_ref=dst.at[rows], send_sem=sems[0].at[j], recv_sem=sems[1].at[j],
            device_id=(to, core), device_id_type=MESH_ID,
        )

    def member_rows(j, i):
        return pl.ds((j * 16 + i) * SLOTS, SLOTS)

    def there_copy(j, i):
        return send(out, arr.at[core], j, member_rows(j, i), (d_send, d_recv), chip_at(j, i, 1))

    def back_copy(j, i):
        return send(total, ret, j, member_rows(j, i), (r_send, r_recv), chip_at(j, i, -1))

    def each(j, act):
        for i in range(16):
            if i == OWN:
                pl.when(j > 0)(lambda: act(j, OWN))
            else:
                act(j, i)

    def all_there(j, count):
        return send(out, arr.at[core], j, pl.ds(0, count * SLOTS), (d_send, d_recv), me)

    def all_back(j, count):
        return send(total, ret, j, pl.ds(0, count * SLOTS), (r_send, r_recv), me)

    def once(j, act):
        pl.when(j == 0)(lambda: act(15))
        pl.when(j > 0)(lambda: act(16))

    own = pl.ds(OWN * SLOTS, SLOTS)

    def dispatch(j, carry):
        place = place_of(j)
        picked = ((slot[0] == place).astype(f32) + (slot[1] == place).astype(f32)).astype(bf16)
        rows = jnp.dot(picked, normed, preferred_element_type=f32)
        tiles[...] = rows.astype(bf16).reshape(PLANE, 16, 128)
        out[pl.ds(j * PLANE, PLANE)] = tiles[...]
        each(j, lambda j, i: there_copy(j, i).start())
        return carry

    lax.fori_loop(0, 4, dispatch, 0)
    arr[core, own] = out[own]
    for load in loads[2:]:
        load.wait()

    def forward(j):
        rows = pl.ds(j * PLANE, PLANE)
        return pltpu.make_async_remote_copy(
            src_ref=arr.at[core, rows], dst_ref=arr.at[core, rows], send_sem=f_send.at[j], recv_sem=f_recv.at[j],
            device_id=(me, other), device_id_type=MESH_ID,
        )

    def partial(j):
        return pltpu.make_async_remote_copy(
            src_ref=part_out.at[j], dst_ref=part_in.at[j], send_sem=p_send.at[j], recv_sem=p_recv.at[j],
            device_id=(me, other), device_id_type=MESH_ID,
        )

    def finish(j):
        partial(j).wait_recv()
        rows = (part[j].astype(f32) + part_in[j].astype(f32)).astype(bf16)
        tiles[...] = rows.reshape(PLANE, 16, 128)
        total[pl.ds(j * PLANE, PLANE)] = tiles[...]

        @pl.when(j == 0)
        def _():
            ret[own] = total[own]

        each(j, lambda j, i: back_copy(j, i).start())

    def receive(j):
        once(j, lambda count: all_there(j, count).wait_recv())
        forward(j).start()

    def unpack_own(j):
        tiles[...] = arr[core, pl.ds(j * PLANE, PLANE)]
        x[0:PLANE, :] = tiles[...].reshape(PLANE, 2048)

    def unpack_other(j):
        rows = pl.ds(j * PLANE, PLANE)
        forward(j).wait_recv()
        tiles[...] = arr[other, rows]
        x[PLANE : 2 * PLANE, :] = tiles[...].reshape(PLANE, 2048)

    receive(jnp.int32(0))
    unpack_own(jnp.int32(0))
    unpack_other(jnp.int32(0))

    def chunk(j, carry):
        def widen(first, end):
            for n in range(first, end):
                at = pl.ds(n * 256, 256)
                g = jnp.dot(x[...], gate[:, at], preferred_element_type=f32)
                u = jnp.dot(x[...], up[:, at], preferred_element_type=f32)
                inner[:, at] = (g / (1.0 + jnp.exp(-g)) * u).astype(bf16)

        widen(0, 3)

        @pl.when(j > 0)
        def _():
            finish(j - 1)

        widen(3, 7)

        @pl.when(j < 3)
        def _():
            receive(j + 1)

        unpack_own(jnp.minimum(j + 1, 3))
        for n in range(8):
            at = pl.ds(n * 256, 256)
            y = jnp.dot(inner[...], down[:, at], preferred_element_type=f32).astype(bf16)
            part[j, :, at] = y[0:PLANE]
            part_out[j, :, at] = y[PLANE : 2 * PLANE]

        partial(j).start()

        @pl.when(j < 3)
        def _():
            unpack_other(j + 1)

        return carry

    lax.fori_loop(0, 4, chunk, 0)
    finish(jnp.int32(3))

    combined[...] = jnp.zeros_like(combined)

    def collect(j, carry):
        once(j, lambda count: all_back(j, count).wait_recv())
        place = place_of(j)
        weight = jnp.where(slot[0] == place, rw_ref[0:1, :], 0.0) + jnp.where(slot[1] == place, rw_ref[1:2, :], 0.0)
        high = weight.astype(bf16)
        low = (weight - high.astype(f32)).astype(bf16)
        tiles[...] = ret[pl.ds(j * PLANE, PLANE)]
        rows = tiles[...].reshape(PLANE, 2048)
        tn = (((0,), (0,)), ((), ()))
        combined[...] += lax.dot_general(high, rows, tn, preferred_element_type=f32) + lax.dot_general(
            low, rows, tn, preferred_element_type=f32
        )
        return carry

    lax.fori_loop(0, 4, collect, 0)
    o_ref[...] = (hidden[...].astype(f32) + rms_scale(combined[...], pfg_ref[...])).astype(bf16)

    def drain(j, carry):
        once(j, lambda count: all_there(j, count).wait_send())
        once(j, lambda count: all_back(j, count).wait_send())
        forward(j).wait_send()
        partial(j).wait_send()
        return carry

    lax.fori_loop(0, 4, drain, 0)


def experts(attended, resid, post_gain, ffn_gain, post_ffn_gain, route_ids, route_w, out_weight, out_weight_other, gate_w, up_w, down_w):
    vmem, hbm = pl.BlockSpec(memory_space=pltpu.VMEM), pl.BlockSpec(memory_space=pltpu.HBM)
    bf16, f32, dma = jnp.bfloat16, jnp.float32, pltpu.SemaphoreType.DMA
    return pl.pallas_call(
        experts_kernel,
        out_shape=jax.ShapeDtypeStruct((128, 2048), bf16),
        in_specs=[vmem] * 7 + [hbm] * 5,
        out_specs=vmem,
        scratch_shapes=[
            pltpu.VMEM((512, 2048), bf16),
            pltpu.VMEM((512, 2048), bf16),
            pltpu.VMEM((2048, 1792), bf16),
            pltpu.VMEM((2048, 1792), bf16),
            pltpu.VMEM((1792, 2048), bf16),
            pltpu.VMEM((128, 512), bf16),
            pltpu.VMEM((128, 2048), bf16),
            pltpu.VMEM((384, 16, 128), bf16),
            pltpu.VMEM((2, 384, 16, 128), bf16),
            pltpu.VMEM((2 * PLANE, 2048), bf16),
            pltpu.VMEM((2 * PLANE, 1792), bf16),
            pltpu.VMEM((4, PLANE, 2048), bf16),
            pltpu.VMEM((4, PLANE, 2048), bf16),
            pltpu.VMEM((4, PLANE, 2048), bf16),
            pltpu.VMEM((384, 16, 128), bf16),
            pltpu.VMEM((384, 16, 128), bf16),
            pltpu.VMEM((128, 2048), f32),
            pltpu.VMEM((PLANE, 16, 128), bf16),
            dma((5,)), dma((2,)), dma((4,)), dma((4,)), dma((4,)), dma((4,)), dma((4,)), dma((4,)),
            dma((4,)), dma((4,)),
        ],
        compiler_params=pltpu.CompilerParams(
            collective_id=1, has_side_effects=True, vmem_limit_bytes=62 << 20
        ),
        cost_estimate=pl.CostEstimate(flops=20_000_000_000, bytes_accessed=28_000_000, transcendentals=0),
        name="experts",
    )(
        attended, resid, post_gain[None], ffn_gain[None], post_ffn_gain[None], route_ids.T, route_w.T,
        out_weight, out_weight_other, gate_w, up_w, down_w,
    )


def per_device(
    queries,
    keys,
    values,
    q_gain,
    k_gain,
    resid,
    out_weight,
    post_gain,
    ffn_gain,
    post_ffn_gain,
    gate_w,
    up_w,
    down_w,
    route_ids,
    route_w,
):
    attended, den, kv, out_weight_other = attention(queries, keys, values, q_gain, k_gain, out_weight)
    attended = lax.cond(
        den[0, 0] < LIMIT,
        lambda: attended,
        lambda: attention_again(queries, q_gain, kv),
    )
    return experts(
        attended, resid, post_gain, ffn_gain, post_ffn_gain, route_ids, route_w, out_weight, out_weight_other,
        gate_w, up_w, down_w,
    )


def solution(mesh):
    in_specs = (
        P("sp", "tp"),
        P("sp", "tp"),
        P("sp", "tp"),
        P(),
        P(),
        P(("sp", "tp"), None),
        P("tp", None),
        P(),
        P(),
        P(),
        P("sp", None, "tp"),
        P("sp", None, "tp"),
        P("sp", "tp", None),
        P(("sp", "tp"), None),
        P(("sp", "tp"), None),
    )
    out_specs = P(("sp", "tp"), None)
    return jax.shard_map(
        per_device, mesh=mesh, in_specs=in_specs, out_specs=out_specs, check_vma=False
    )
```
